32 devices in a mesh: grp: 1, fs: 2 (over x), tp: 16 (over z, y, core).
Axes of the slice: x: 2, y: 2, z: 4, core: 2. Of those that a mesh axis runs over, the one named last changes fastest.
Arguments:
- prompt_rows: bfloat16 [512, 2048], P(('grp', 'fs')), may hold values from -6 to 6
- gain_before: float32 [2048], P('fs'), may hold values from 0.1 to 1.9
- gate_before: float32 [2048, 5632], P('fs', 'tp'), may hold values from -0.125 to 0.125
- up_before: float32 [2048, 5632], P('fs', 'tp'), may hold values from -0.125 to 0.125
- down_before: float32 [5632, 2048], P('fs', 'tp'), may hold values from -0.3125 to 0.3125
- gain_after: float32 [2048], P('fs'), may hold values from 0.1 to 1.9
- gate_after: float32 [2048, 5632], P('fs', 'tp'), may hold values from -0.125 to 0.125
- up_after: float32 [2048, 5632], P('fs', 'tp'), may hold values from -0.125 to 0.125
- down_after: float32 [5632, 2048], P('fs', 'tp'), may hold values from -0.3125 to 0.3125
Outputs:
- mixed_rows: bfloat16 [512, 2048], P(('grp', 'fs'))
- served_gate_before: bfloat16 [2048, 5632], P('grp', 'tp')
- served_up_before: bfloat16 [2048, 5632], P('grp', 'tp')
- served_down_before: bfloat16 [5632, 2048], P(('grp', 'tp'))
- served_gate_after: bfloat16 [2048, 5632], P('grp', 'tp')
- served_up_after: bfloat16 [2048, 5632], P('grp', 'tp')
- served_down_after: bfloat16 [5632, 2048], P(('grp', 'tp'))
The draws below stay inside these ranges and needn't reach their ends.
All inputs are finite; a program needn't handle non-finite values.
Results may differ from the reference program's by a relative error of at most 0.03.
Values may be sent and summed in bfloat16 or wider, within the bound.
A program may use at most 64 MiB of HBM per device.

```python
import jax
import jax.numpy as jnp
from jax import lax

D = 2048
FF = 5632
TOKENS = 512
N_TP = 16


def levels(own_key, extent, cuts, least, largest):
    level, own = 1.0, jax.random.fold_in(own_key, 6)
    for position, shards_of in cuts:
        draws = jnp.exp(jax.random.uniform(jax.random.fold_in(own, position), (shards_of,), jnp.float32, least / len(cuts), largest / len(cuts)))
        level = level * jnp.repeat(draws, extent[position] // shards_of).reshape([-1 if axis == position else 1 for axis in range(len(extent))])
    return level


def scatter_about(rng, extent, spread, bound, pieces=(), kind=jnp.bfloat16):
    entries = spread * jax.random.normal(rng, extent, jnp.float32)
    if pieces:
        entries = entries * levels(rng, extent, pieces, -0.22, 0.18)
    return jnp.clip(entries, -bound, bound).astype(kind)


def setup_inputs(seed: int = 0, part: int = 0) -> dict:
    key_list = jax.random.split(jax.random.key(seed), 10)
    part_splits = jax.random.split(jax.random.fold_in(key_list[9], part), 10)
    return {
        "prompt_rows": scatter_about(part_splits[0], (TOKENS, D), 1.0, 6.0, ((0, 2),)),
        "gain_before": jnp.clip(1.0 + 0.18 * jax.random.normal(key_list[1], (D,), jnp.float32), 0.1, 1.9),
        "gate_before": scatter_about(key_list[2], (D, FF), D ** -0.5, 0.125, ((0, 2), (1, 16)), jnp.float32),
        "up_before": scatter_about(key_list[3], (D, FF), D ** -0.5, 0.125, ((0, 2), (1, 16)), jnp.float32),
        "down_before": scatter_about(key_list[4], (FF, D), (FF // 16) ** -0.5, 0.3125, ((0, 2), (1, 16)), jnp.float32),
        "gain_after": jnp.clip(1.0 + 0.18 * jax.random.normal(key_list[5], (D,), jnp.float32), 0.1, 1.9),
        "gate_after": scatter_about(key_list[6], (D, FF), D ** -0.5, 0.125, ((0, 2), (1, 16)), jnp.float32),
        "up_after": scatter_about(key_list[7], (D, FF), D ** -0.5, 0.125, ((0, 2), (1, 16)), jnp.float32),
        "down_after": scatter_about(key_list[8], (FF, D), (FF // 16) ** -0.5, 0.3125, ((0, 2), (1, 16)), jnp.float32),
    }


EPS = 1e-06

def fold(gain, gate_w, up_w, down_w):
    served_gate = (gain[:, None] * gate_w).astype(jnp.bfloat16)
    served_up = (gain[:, None] * up_w).astype(jnp.bfloat16)
    return (served_gate, served_up, down_w.astype(jnp.bfloat16))

def half_step(row_block, gate_w, up_w, down_w):
    values = row_block.astype(jnp.float32)
    normed = (values * lax.rsqrt(lax.optimization_barrier(jnp.mean(values * values, axis=-1, keepdims=True)) + EPS)).astype(jnp.bfloat16)
    gate_pre = jnp.dot(normed, gate_w, preferred_element_type=jnp.float32)
    up_pre = jnp.dot(normed, up_w, preferred_element_type=jnp.float32)
    hidden = (jax.nn.silu(gate_pre) * up_pre).astype(jnp.bfloat16)
    width = FF // N_TP
    hidden_blocks = hidden.reshape(hidden.shape[0], N_TP, width).transpose(1, 0, 2)
    down_blocks = down_w.reshape(N_TP, width, D)

    def add_block(total, pair):
        part_sum = jnp.dot(pair[0], pair[1], preferred_element_type=jnp.float32).astype(jnp.bfloat16)
        part_sum = lax.optimization_barrier(part_sum)
        return (total + part_sum.astype(jnp.float32), None)
    total, _ = lax.scan(add_block, jnp.zeros((hidden.shape[0], D), jnp.float32), (hidden_blocks, down_blocks))
    return (values + 0.5 * total).astype(jnp.bfloat16)

def reference(prompt_rows, gain_before, gate_before, up_before, down_before, gain_after, gate_after, up_after, down_after):
    gate_one, up_one, down_one = fold(gain_before, gate_before, up_before, down_before)
    gate_two, up_two, down_two = fold(gain_after, gate_after, up_after, down_after)
    middle = half_step(prompt_rows, gate_one, up_one, down_one)
    mixed = half_step(middle, gate_two, up_two, down_two)
    return (mixed, gate_one, up_one, down_one, gate_two, up_two, down_two)
```

```python
import functools

import jax
import jax.numpy as jnp
from jax import lax
from jax.experimental import pallas as pl
from jax.experimental.pallas import tpu as pltpu
from jax.sharding import PartitionSpec as P

MESH = pl.DeviceIdType.MESH
BF16 = jnp.bfloat16
F32 = jnp.float32

EPS = 1e-06


def serve_weights(gain, gate_w, up_w, down_w):
    gate_half = (gain[:, None] * gate_w).astype(jnp.bfloat16)
    up_half = (gain[:, None] * up_w).astype(jnp.bfloat16)
    down_half = down_w.astype(jnp.bfloat16)
    gate_whole, up_whole = (
        lax.all_gather(gate_half, "fs", axis=0, tiled=True),
        lax.all_gather(up_half, "fs", axis=0, tiled=True),
    )
    tall_block = lax.all_gather(down_half, "fs", axis=0, tiled=True)
    down_whole = lax.all_to_all(tall_block, "tp", split_axis=0, concat_axis=1, tiled=True)
    return (gate_whole, up_whole, down_whole)


def half_step(row_block, gate_w, up_w, down_w):
    values = row_block.astype(jnp.float32)
    normed = (values * lax.rsqrt(jnp.mean(values * values, axis=-1, keepdims=True) + EPS)).astype(
        jnp.bfloat16
    )
    gate_pre = jnp.dot(normed, gate_w, preferred_element_type=jnp.float32)
    up_pre = jnp.dot(normed, up_w, preferred_element_type=jnp.float32)
    hidden = (jax.nn.silu(gate_pre) * up_pre).astype(jnp.bfloat16)
    total = lax.psum(
        jnp.dot(hidden, down_w, preferred_element_type=jnp.float32).astype(jnp.bfloat16), "tp"
    ).astype(jnp.float32)
    return (values + 0.5 * total).astype(jnp.bfloat16)


def body(
    prompt_rows,
    gain_before,
    gate_before,
    up_before,
    down_before,
    gain_after,
    gate_after,
    up_after,
    down_after,
):
    gate_one, up_one, down_one = serve_weights(gain_before, gate_before, up_before, down_before)
    gate_two, up_two, down_two = serve_weights(gain_after, gate_after, up_after, down_after)
    middle = half_step(prompt_rows, gate_one, up_one, down_one)
    mixed = half_step(middle, gate_two, up_two, down_two)
    return (mixed, gate_one, up_one, down_one, gate_two, up_two, down_two)


def rows_of(start, size, unit):
    return pl.ds(pl.multiple_of(start, unit), size)


def kernel(
    n_tp,
    x_hbm, gain1_hbm, gate1_hbm, up1_hbm, down1_hbm, gain2_hbm, gate2_hbm, up2_hbm, down2_hbm,
    mixed, gate1, up1, down1, gate2, up2, down2,
    x, gain, wide, tall_in, tall, normed, hidden, part, pair, ysend, yrecv, zsend, zrecv, middle,
    in_sem, x_send, x_recv, a_send, a_recv, p_send, p_recv, y_send, y_recv, s_send, s_recv,
    g_send, g_recv, b_send, h_send, h_recv,
):
    f = lax.axis_index("fs")
    t = lax.axis_index("tp")
    other = 1 - f
    core = lax.rem(t, 2)
    chip = t // 2
    sibling = t + 1 - 2 * core
    chips = n_tp // 2
    width, depth = wide.shape[1:]
    tall_half = tall_in.shape[1]
    served = (gate1, up1, gate2, up2)
    down = (down1, down2)
    block = down1.shape[0]
    col = tall.shape[2]
    tokens = x.shape[0]
    side = tokens // 2
    piece = side // chips
    per_half = n_tp // 2
    lanes = chips // 2
    far = chip // 2
    lane = lax.rem(chip, 2)

    loads = {}
    sources = (
        ("down1", down1_hbm, tall_in.at[0]), ("gain1", gain1_hbm, gain.at[0]),
        ("gate1", gate1_hbm, wide.at[0]), ("up1", up1_hbm, wide.at[1]),
        ("down2", down2_hbm, tall_in.at[1]), ("gain2", gain2_hbm, gain.at[1]),
        ("gate2", gate2_hbm, wide.at[2]), ("up2", up2_hbm, wide.at[3]), ("x", x_hbm, x),
    )
    for i, (name, src, dst) in enumerate(sources):
        loads[name] = pltpu.make_async_copy(src, dst, in_sem.at[i])
        loads[name].start()

    barrier = pltpu.get_barrier_semaphore()
    for k in range(1, n_tp):
        pl.semaphore_signal(
            barrier, inc=1, device_id={"fs": f, "tp": lax.rem(t + k, n_tp)}, device_id_type=MESH
        )
    pl.semaphore_signal(barrier, inc=1, device_id={"fs": other, "tp": t}, device_id_type=MESH)
    pl.semaphore_wait(barrier, n_tp)

    def across(ref, slot):
        return pltpu.make_async_remote_copy(
            src_ref=ref, dst_ref=ref, send_sem=x_send.at[slot], recv_sem=x_recv.at[slot],
            device_id={"fs": other, "tp": t}, device_id_type=MESH,
        )

    near = rows_of(f * depth, depth, depth)

    def fold_wide(i, gain_slot):
        def one(k, _):
            rows = rows_of(k * 32, 32, 32)
            served[i][rows, near] = (gain[gain_slot] * wide[i, rows, :]).astype(BF16)
            return 0

        lax.fori_loop(0, width // 32, one, 0)
        return across(served[i].at[:, near], i)

    def fold_tall(layer):
        step = tall_half // 8

        def one(k, _):
            tall[layer, rows_of(f * tall_half + k * step, step, 16), :] = tall_in[
                layer, rows_of(k * step, step, 16), :
            ].astype(BF16)
            return 0

        lax.fori_loop(0, 8, one, 0)
        return across(tall.at[layer, rows_of(f * tall_half, tall_half, 16)], 4 + layer)

    my_cols = pl.ds(pl.multiple_of(t * col, col), col)

    def block_copy(layer, b, sender):
        return pltpu.make_async_remote_copy(
            src_ref=tall.at[layer, rows_of(b * block, block, 16)],
            dst_ref=down[layer].at[:, my_cols],
            send_sem=a_send.at[layer, b], recv_sem=a_recv.at[layer, sender],
            device_id={"fs": f, "tp": b}, device_id_type=MESH,
        )

    def hand_out(layer, which):
        def one(k, _):
            b = which * per_half + lax.rem(t + k, per_half)

            @pl.when(b != t)
            def _():
                block_copy(layer, b, t).start()

            return 0

        lax.fori_loop(0, per_half, one, 0)

    def collect(layer):
        def one(k, _):
            block_copy(layer, t, lax.rem(t + k, n_tp)).wait_recv()
            return 0

        lax.fori_loop(1, n_tp, one, 0)
        down[layer][:, my_cols] = tall[layer, rows_of(t * block, block, 16), :]

    sends = []
    loads["down1"].wait()
    tall_one = fold_tall(0)
    tall_one.start()
    hand_out(0, f)
    loads["down2"].wait()
    tall_two = fold_tall(1)
    tall_two.start()
    hand_out(1, f)
    loads["gain1"].wait()
    loads["gate1"].wait()
    gate_one = fold_wide(0, 0)
    loads["up1"].wait()
    up_one = fold_wide(1, 0)
    loads["gain2"].wait()
    loads["gate2"].wait()
    gate_two = fold_wide(2, 1)
    loads["up2"].wait()
    up_two = fold_wide(3, 1)
    loads["x"].wait()

    def unit(v):
        return (v * lax.rsqrt(jnp.mean(v * v, axis=-1, keepdims=True) + EPS)).astype(BF16)

    def norm(k, _):
        rows = rows_of(k * 32, 32, 32)
        normed[0, rows, :] = unit(x[rows, :].astype(F32))
        return 0

    lax.fori_loop(0, tokens // 32, norm, 0)
    tall_one.wait_recv()
    gate_one.start()
    hand_out(0, other)
    tall_two.wait_recv()
    up_one.start()
    hand_out(1, other)

    turned = (((1,), (1,)), ((), ()))

    def hide(layer):
        gate, up = served[2 * layer], served[2 * layer + 1]
        step = tokens // 2

        def one(k, _):
            rows = rows_of(k * step, step, step)
            v = normed[layer, rows, :]
            g = lax.dot_general(v, gate[...], turned, preferred_element_type=F32)
            u = lax.dot_general(v, up[...], turned, preferred_element_type=F32)
            hidden[rows, :] = (g / (1.0 + jnp.exp(-g)) * u).astype(BF16)
            return 0

        lax.fori_loop(0, 2, one, 0)

    def spot(z, y):
        return (y * lanes + z) * piece

    def rows_at(c, z, y):
        return rows_of(c * side + spot(z, y), piece, piece)

    def to(tp, src, dst, send, recv):
        return pltpu.make_async_remote_copy(
            src_ref=src, dst_ref=dst, send_sem=send, recv_sem=recv,
            device_id={"fs": f, "tp": tp}, device_id_type=MESH,
        )

    beside = 2 * (2 * far + 1 - lane) + core

    def at_far(z):
        return 2 * (2 * z + lane) + core

    def swap(layer, y):
        half = side // 2
        src = part.at[layer, rows_of((1 - core) * side + y * half, half, half)]
        return to(sibling, src, pair.at[layer, rows_of(y * half, half, half)],
                  p_send.at[layer, y], p_recv.at[layer, y])

    def y_copy(layer, z):
        return to(beside, ysend.at[layer, z], yrecv.at[layer, z], y_send.at[layer, z], y_recv.at[layer, z])

    def z_copy(layer, z, sender):
        return to(at_far(z), zsend.at[layer, z], zrecv.at[layer, sender],
                  s_send.at[layer, z], s_recv.at[layer, sender])

    own = rows_at(core, far, lane)

    def project(layer):
        def rows_for(c):
            rows = rows_of(c * side, side, side)
            p = jnp.dot(hidden[rows, :], down[layer][...], preferred_element_type=F32)
            part[layer, rows, :] = p.astype(BF16)

        rows_for(1 - core)
        swap(layer, 1 - lane).start()
        swap(layer, lane).start()
        rows_for(core)

    def two(layer, z, y):
        return part[layer, rows_at(core, z, y), :].astype(F32) + pair[
            layer, rows_of(spot(z, y), piece, piece), :
        ].astype(F32)

    def reduce(layer):
        swap(layer, 1 - lane).wait_recv()

        def step_y(k, _):
            z = lax.rem(far + k, lanes)
            ysend[layer, z] = two(layer, z, 1 - lane).astype(BF16)
            y_copy(layer, z).start()
            return 0

        lax.fori_loop(1, lanes + 1, step_y, 0)
        swap(layer, lane).wait_recv()

        def step_z(k, _):
            z = lax.rem(far + k, lanes)
            y_copy(layer, z).wait_recv()
            zsend[layer, z] = (two(layer, z, lane) + yrecv[layer, z].astype(F32)).astype(BF16)
            z_copy(layer, z, far).start()
            return 0

        lax.fori_loop(1, lanes, step_z, 0)
        y_copy(layer, far).wait_recv()
        total = two(layer, far, lane) + yrecv[layer, far].astype(F32)
        for k in range(1, lanes):
            z = lax.rem(far + lanes - k, lanes)
            z_copy(layer, far, z).wait_recv()
            total = total + zrecv[layer, z].astype(F32)
        return total

    def gathered(layer):
        return mixed if layer else normed.at[1]

    def piece_copy(layer, z, y, device, send):
        ref = gathered(layer).at[rows_at(core, z, y)]
        return to(device, ref, ref, send, g_recv.at[layer, 2 * z + y])

    def z_piece(layer, z, owner):
        return piece_copy(layer, owner, lane, at_far(z), g_send.at[layer, z])

    def y_piece(layer, z, y):
        return piece_copy(layer, z, y, beside, b_send.at[layer, z])

    def core_piece(layer, z, y, c):
        ref = gathered(layer).at[rows_at(c, z, y)]
        return to(sibling, ref, ref, h_send.at[layer, 2 * z + y], h_recv.at[layer, 2 * z + y])

    def gather(layer):
        def send_z(k, _):
            z_piece(layer, lax.rem(far + k, lanes), far).start()
            return 0

        lax.fori_loop(1, lanes, send_z, 0)
        y_piece(layer, far, lane).start()
        core_piece(layer, far, lane, core).start()

        def pass_z(k, _):
            z = lax.rem(far + lanes - k, lanes)
            z_piece(layer, far, z).wait_recv()
            y_piece(layer, z, lane).start()
            core_piece(layer, z, lane, core).start()
            return 0

        lax.fori_loop(1, lanes, pass_z, 0)

        def pass_y(k, _):
            z = lax.rem(far + lanes - k, lanes)
            y_piece(layer, z, 1 - lane).wait_recv()
            core_piece(layer, z, 1 - lane, core).start()
            return 0

        lax.fori_loop(0, lanes, pass_y, 0)

        def land(k, _):
            core_piece(layer, k // 2, lax.rem(k, 2), 1 - core).wait_recv()
            return 0

        lax.fori_loop(0, chips, land, 0)

    gate_one.wait_recv()
    gate_two.start()
    up_one.wait_recv()
    up_two.start()
    hide(0)
    collect(0)
    project(0)
    total = reduce(0)
    value = (x[own, :].astype(F32) + 0.5 * total).astype(BF16)
    middle[...] = value
    normed[1, own, :] = unit(value.astype(F32))
    gather(0)
    gate_two.wait_recv()
    up_two.wait_recv()
    hide(1)
    collect(1)
    project(1)
    total = reduce(1)
    mixed[own, :] = (middle[...].astype(F32) + 0.5 * total).astype(BF16)
    gather(1)

    for sent in (tall_one, gate_one, up_one, tall_two, gate_two, up_two):
        sent.wait_send()
    for layer in range(2):

        def drain(k, _):
            block_copy(layer, lax.rem(t + k, n_tp), t).wait_send()
            return 0

        lax.fori_loop(1, n_tp, drain, 0)
        swap(layer, 0).wait_send()
        swap(layer, 1).wait_send()

        def drain_z(k, _):
            z = lax.rem(far + k, lanes)
            z_copy(layer, z, far).wait_send()
            z_piece(layer, z, far).wait_send()
            return 0

        lax.fori_loop(1, lanes, drain_z, 0)

        def drain_y(z, _):
            y_copy(layer, z).wait_send()
            y_piece(layer, z, lane).wait_send()
            return 0

        lax.fori_loop(0, lanes, drain_y, 0)

        def drain_c(k, _):
            core_piece(layer, k // 2, lax.rem(k, 2), core).wait_send()
            return 0

        lax.fori_loop(0, chips, drain_c, 0)


def flush(*refs):
    n = len(refs) // 2
    copies = [
        pltpu.make_async_copy(src, dst, refs[-1].at[i])
        for i, (src, dst) in enumerate(zip(refs[:n], refs[n : 2 * n]))
    ]
    for copy in copies:
        copy.start()
    for copy in copies:
        copy.wait()


def fused(n_tp, x, gain1, gate1, up1, down1, gain2, gate2, up2, down2):
    depth, width = gate1.shape
    tall_half, col = down1.shape
    tokens, model = x.shape
    block = 2 * tall_half // n_tp
    chips = n_tp // 2
    lanes = chips // 2
    side = tokens // 2
    piece = side // chips
    dma = pltpu.SemaphoreType.DMA
    vmem = pltpu.VMEM
    anywhere = pl.BlockSpec(memory_space=pl.ANY)
    wide_out = vmem((width, 2 * depth), BF16)
    down_out = vmem((block, model), BF16)
    held = pl.pallas_call(
        functools.partial(kernel, n_tp),
        out_shape=(vmem(x.shape, BF16), wide_out, wide_out, down_out, wide_out, wide_out, down_out),
        in_specs=[anywhere] * 9,
        out_specs=[pl.BlockSpec(memory_space=pltpu.VMEM)] * 7,
        scratch_shapes=[
            vmem((tokens, model), BF16),
            vmem((2, 1, depth), F32),
            vmem((4, width, depth), F32),
            vmem((2, tall_half, col), F32),
            vmem((2, 2 * tall_half, col), BF16),
            vmem((2, tokens, model), BF16),
            vmem((tokens, width), BF16),
            vmem((2, tokens, model), BF16),
            vmem((2, side, model), BF16),
            vmem((2, lanes, piece, model), BF16),
            vmem((2, lanes, piece, model), BF16),
            vmem((2, lanes, piece, model), BF16),
            vmem((2, lanes, piece, model), BF16),
            vmem((piece, model), BF16),
            dma((9,)), dma((6,)), dma((6,)), dma((2, n_tp)), dma((2, n_tp)),
            dma((2, 2)), dma((2, 2)), dma((2, lanes)), dma((2, lanes)), dma((2, lanes)), dma((2, lanes)),
            dma((2, lanes)), dma((2, chips)), dma((2, lanes)), dma((2, chips)), dma((2, chips)),
        ],
        compiler_params=pltpu.CompilerParams(
            collective_id=0, has_side_effects=True, vmem_limit_bytes=54 * 1024 * 1024
        ),
        name="hand_over",
    )(x, gain1[None, :], gate1.T, up1.T, down1, gain2[None, :], gate2.T, up2.T, down2)
    mixed, gate_one, up_one, down_one, gate_two, up_two, down_two = pl.pallas_call(
        flush,
        out_shape=tuple(jax.ShapeDtypeStruct(v.shape, v.dtype) for v in held),
        in_specs=[anywhere] * 7,
        out_specs=[anywhere] * 7,
        scratch_shapes=[dma((7,))],
        compiler_params=pltpu.CompilerParams(vmem_limit_bytes=1024 * 1024),
        name="flush",
    )(*held)
    return (mixed, gate_one.T, up_one.T, down_one, gate_two.T, up_two.T, down_two)


def solution(mesh):
    placed = (
        P(("grp", "fs"), None),
        P("fs"),
        P("fs", "tp"),
        P("fs", "tp"),
        P("fs", "tp"),
        P("fs"),
        P("fs", "tp"),
        P("fs", "tp"),
        P("fs", "tp"),
    )
    paired = mesh.shape["fs"] == 2 and mesh.shape["tp"] % 4 == 0
    return jax.shard_map(
        functools.partial(fused, mesh.shape["tp"]) if paired else body,
        mesh=mesh,
        in_specs=placed,
        out_specs=(
            P(("grp", "fs"), None),
            P("grp", "tp"),
            P("grp", "tp"),
            P(("grp", "tp"), None),
            P("grp", "tp"),
            P("grp", "tp"),
            P(("grp", "tp"), None),
        ),
        check_vma=False,
    )
```

```python
import functools

import jax
import jax.numpy as jnp
from jax import lax
from jax.experimental import pallas as pl
from jax.experimental.pallas import tpu as pltpu
from jax.sharding import PartitionSpec as P

MESH = pl.DeviceIdType.MESH
BF16 = jnp.bfloat16
F32 = jnp.float32

EPS = 1e-06


def serve_weights(gain, gate_w, up_w, down_w):
    gate_half = (gain[:, None] * gate_w).astype(jnp.bfloat16)
    up_half = (gain[:, None] * up_w).astype(jnp.bfloat16)
    down_half = down_w.astype(jnp.bfloat16)
    gate_whole, up_whole = (
        lax.all_gather(gate_half, "fs", axis=0, tiled=True),
        lax.all_gather(up_half, "fs", axis=0, tiled=True),
    )
    tall_block = lax.all_gather(down_half, "fs", axis=0, tiled=True)
    down_whole = lax.all_to_all(tall_block, "tp", split_axis=0, concat_axis=1, tiled=True)
    return (gate_whole, up_whole, down_whole)


def half_step(row_block, gate_w, up_w, down_w):
    values = row_block.astype(jnp.float32)
    normed = (values * lax.rsqrt(jnp.mean(values * values, axis=-1, keepdims=True) + EPS)).astype(
        jnp.bfloat16
    )
    gate_pre = jnp.dot(normed, gate_w, preferred_element_type=jnp.float32)
    up_pre = jnp.dot(normed, up_w, preferred_element_type=jnp.float32)
    hidden = (jax.nn.silu(gate_pre) * up_pre).astype(jnp.bfloat16)
    total = lax.psum(
        jnp.dot(hidden, down_w, preferred_element_type=jnp.float32).astype(jnp.bfloat16), "tp"
    ).astype(jnp.float32)
    return (values + 0.5 * total).astype(jnp.bfloat16)


def body(
    prompt_rows,
    gain_before,
    gate_before,
    up_before,
    down_before,
    gain_after,
    gate_after,
    up_after,
    down_after,
):
    gate_one, up_one, down_one = serve_weights(gain_before, gate_before, up_before, down_before)
    gate_two, up_two, down_two = serve_weights(gain_after, gate_after, up_after, down_after)
    middle = half_step(prompt_rows, gate_one, up_one, down_one)
    mixed = half_step(middle, gate_two, up_two, down_two)
    return (mixed, gate_one, up_one, down_one, gate_two, up_two, down_two)


def rows_of(start, size, unit):
    return pl.ds(pl.multiple_of(start, unit), size)


def kernel(
    n_tp,
    x_hbm, gain1_hbm, gate1_hbm, up1_hbm, down1_hbm, gain2_hbm, gate2_hbm, up2_hbm, down2_hbm,
    mixed, gate1, up1, down1, gate2, up2, down2,
    x, gain, wide, tall_in, tall, normed, guest, psend, precv, kept, hidden, part, pair,
    ysend, yrecv, zsend, zrecv, middle,
    in_sem, x_send, x_recv, d_send, d_recv, v_send, v_recv, a_send, a_recv, p_send, p_recv, y_send, y_recv, s_send, s_recv,
    g_send, g_recv, b_send, h_send, h_recv,
):
    f = lax.axis_index("fs")
    t = lax.axis_index("tp")
    other = 1 - f
    core = lax.rem(t, 2)
    chip = t // 2
    sibling = t + 1 - 2 * core
    chips = n_tp // 2
    width, depth = wide.shape[1:]
    tall_half = tall_in.shape[1]
    served = (gate1, up1, gate2, up2)
    down = (down1, down2)
    block = down1.shape[0]
    col = tall.shape[2]
    tokens = x.shape[0]
    side = tokens // 2
    piece = side // chips
    per_half = n_tp // 2
    lanes = chips // 2
    far = chip // 2
    lane = lax.rem(chip, 2)

    loads = {}
    sources = (
        ("x", x_hbm, x), ("down1", down1_hbm, tall_in.at[0]), ("gain1", gain1_hbm, gain.at[0]),
        ("gate1", gate1_hbm, wide.at[0]), ("up1", up1_hbm, wide.at[1]),
        ("down2", down2_hbm, tall_in.at[1]), ("gain2", gain2_hbm, gain.at[1]),
        ("gate2", gate2_hbm, wide.at[2]), ("up2", up2_hbm, wide.at[3]),
    )
    for i, (name, src, dst) in enumerate(sources):
        loads[name] = pltpu.make_async_copy(src, dst, in_sem.at[i])
        loads[name].start()

    barrier = pltpu.get_barrier_semaphore()
    for k in range(1, n_tp):
        pl.semaphore_signal(
            barrier, inc=1, device_id={"fs": f, "tp": lax.rem(t + k, n_tp)}, device_id_type=MESH
        )
    pl.semaphore_signal(barrier, inc=1, device_id={"fs": other, "tp": t}, device_id_type=MESH)
    def unit(v):
        return (v * lax.rsqrt(jnp.mean(v * v, axis=-1, keepdims=True) + EPS)).astype(BF16)

    def norm(k, _):
        rows = rows_of(k * 32, 32, 32)
        normed[0, rows, :] = unit(x[rows, :].astype(F32))
        return 0

    loads["x"].wait()
    lax.fori_loop(0, tokens // 32, norm, 0)

    near = rows_of(f * depth, depth, depth)
    away = rows_of(other * depth, depth, depth)

    def across(src, dst, send, recv):
        return pltpu.make_async_remote_copy(
            src_ref=src, dst_ref=dst, send_sem=send, recv_sem=recv,
            device_id={"fs": other, "tp": t}, device_id_type=MESH,
        )

    def to(tp, src, dst, send, recv):
        return pltpu.make_async_remote_copy(
            src_ref=src, dst_ref=dst, send_sem=send, recv_sem=recv,
            device_id={"fs": f, "tp": tp}, device_id_type=MESH,
        )

    def wide_copy(i):
        ref = served[i].at[:, near]
        return across(ref, ref, x_send.at[i], x_recv.at[i])

    def fold_wide(i, gain_slot):
        def one(k, _):
            rows = rows_of(k * 32, 32, 32)
            served[i][rows, near] = (gain[gain_slot] * wide[i, rows, :]).astype(BF16)
            return 0

        lax.fori_loop(0, width // 32, one, 0)

    def fold_tall(layer):
        step = tall_half // 8

        def one(k, _):
            tall[layer, rows_of(f * tall_half + k * step, step, 16), :] = tall_in[
                layer, rows_of(k * step, step, 16), :
            ].astype(BF16)
            return 0

        lax.fori_loop(0, 8, one, 0)

    my_cols = pl.ds(pl.multiple_of(t * col, col), col)

    def block_copy(layer, b, sender):
        return to(
            b, tall.at[layer, rows_of(b * block, block, 16)], down[layer].at[:, my_cols],
            a_send.at[layer, b], a_recv.at[layer, sender],
        )

    def tall_copy(layer, b):
        ref = tall.at[layer, rows_of(b * block, block, 16)]
        return across(ref, ref, d_send.at[layer, b], d_recv.at[layer, b])

    def turn(which, k):
        return which * per_half + lax.rem(t + k, per_half)

    def cross_tall(layer):
        def one(k, _):
            tall_copy(layer, turn(f, k)).start()
            return 0

        lax.fori_loop(0, per_half, one, 0)

    def hand_out(layer, first, last):
        def one(k, _):
            b = turn(f, k)

            @pl.when(b != t)
            def _():
                block_copy(layer, b, t).start()

            return 0

        lax.fori_loop(first, last, one, 0)

    def pass_on(layer, first, last):
        def one(k, _):
            b = turn(other, k)
            tall_copy(layer, b).wait_recv()

            @pl.when(b != t)
            def _():
                block_copy(layer, b, t).start()

            return 0

        lax.fori_loop(first, last, one, 0)

    def collect(layer):
        def one(k, _):
            block_copy(layer, t, lax.rem(t + k, n_tp)).wait_recv()
            return 0

        lax.fori_loop(1, n_tp, one, 0)
        down[layer][:, my_cols] = tall[layer, rows_of(t * block, block, 16), :]

    beside = 2 * (2 * far + 1 - lane) + core
    quarter = tokens // 4

    def share(y, c):
        return rows_of((2 * y + c) * quarter, quarter, quarter)

    guest_in = across(
        normed.at[0, share(lane, core), away], guest.at[share(lane, core)], v_send.at[0], v_recv.at[0]
    )

    def guest_copy(device, y, c, slot):
        ref = guest.at[share(y, c)]
        return to(device, ref, ref, v_send.at[slot], v_recv.at[slot])

    loads["down1"].wait()
    fold_tall(0)
    pl.semaphore_wait(barrier, n_tp)
    guest_in.start()
    cross_tall(0)
    hand_out(0, 0, per_half)
    loads["gain1"].wait()
    loads["gate1"].wait()
    fold_wide(0, 0)
    loads["up1"].wait()
    fold_wide(1, 0)
    guest_in.wait_recv()
    guest_copy(beside, lane, core, 1).start()
    guest_copy(sibling, lane, core, 2).start()
    loads["down2"].wait()
    fold_tall(1)
    pass_on(0, 0, 1)
    guest_copy(beside, 1 - lane, core, 1).wait_recv()
    guest_copy(sibling, 1 - lane, core, 3).start()
    loads["gain2"].wait()
    loads["gate2"].wait()
    fold_wide(2, 1)
    loads["up2"].wait()
    fold_wide(3, 1)
    guest_copy(sibling, lane, 1 - core, 2).wait_recv()
    guest_copy(sibling, 1 - lane, 1 - core, 3).wait_recv()

    turned = (((1,), (1,)), ((), ()))

    def times(rows, i, cols):
        return lax.dot_general(rows, served[i][:, cols], turned, preferred_element_type=F32)

    def partial_copy(i):
        return across(psend.at[i], precv.at[i], v_send.at[4 + i], v_recv.at[4 + i])

    for i in range(2):
        psend[i] = times(guest[...], i, near).astype(BF16)
        partial_copy(i).start()
    cross_tall(1)
    for i in (2, 3, 0, 1):
        wide_copy(i).start()
    pass_on(0, 1, 3)
    for i in range(2):
        kept[i] = times(normed[0, :, near], i, near)
    pass_on(0, 3, per_half)

    def gated(rows, g, u):
        hidden[rows, :] = (g / (1.0 + jnp.exp(-g)) * u).astype(BF16)

    def hide_one():
        def one(k, _):
            rows = rows_of(k * 32, 32, 32)
            gated(rows, kept[0, rows, :] + precv[0, rows, :].astype(F32),
                  kept[1, rows, :] + precv[1, rows, :].astype(F32))
            return 0

        lax.fori_loop(0, tokens // 32, one, 0)

    def hide_two():
        step = tokens // 2

        def one(k, _):
            rows = rows_of(k * step, step, step)
            v = normed[1, rows, :]
            g = lax.dot_general(v, gate2[...], turned, preferred_element_type=F32)
            u = lax.dot_general(v, up2[...], turned, preferred_element_type=F32)
            gated(rows, g, u)
            return 0

        lax.fori_loop(0, 2, one, 0)

    def spot(z, y):
        return (y * lanes + z) * piece

    def rows_at(c, z, y):
        return rows_of(c * side + spot(z, y), piece, piece)

    def at_far(z):
        return 2 * (2 * z + lane) + core

    def swap(layer, y):
        half = side // 2
        src = part.at[layer, rows_of((1 - core) * side + y * half, half, half)]
        return to(sibling, src, pair.at[layer, rows_of(y * half, half, half)],
                  p_send.at[layer, y], p_recv.at[layer, y])

    def y_copy(layer, z):
        return to(beside, ysend.at[layer, z], yrecv.at[layer, z], y_send.at[layer, z], y_recv.at[layer, z])

    def z_copy(layer, z, sender):
        return to(at_far(z), zsend.at[layer, z], zrecv.at[layer, sender],
                  s_send.at[layer, z], s_recv.at[layer, sender])

    own = rows_at(core, far, lane)

    def project(layer):
        def rows_for(c):
            rows = rows_of(c * side, side, side)
            p = jnp.dot(hidden[rows, :], down[layer][...], preferred_element_type=F32)
            part[layer, rows, :] = p.astype(BF16)

        rows_for(1 - core)
        swap(layer, 1 - lane).start()
        swap(layer, lane).start()
        rows_for(core)

    def two(layer, z, y):
        return part[layer, rows_at(core, z, y), :].astype(F32) + pair[
            layer, rows_of(spot(z, y), piece, piece), :
        ].astype(F32)

    def reduce(layer, then):
        swap(layer, 1 - lane).wait_recv()

        def step_y(k, _):
            z = lax.rem(far + k, lanes)
            ysend[layer, z] = two(layer, z, 1 - lane).astype(BF16)
            y_copy(layer, z).start()
            return 0

        lax.fori_loop(1, lanes + 1, step_y, 0)
        swap(layer, lane).wait_recv()

        def step_z(k, _):
            z = lax.rem(far + k, lanes)
            y_copy(layer, z).wait_recv()
            zsend[layer, z] = (two(layer, z, lane) + yrecv[layer, z].astype(F32)).astype(BF16)
            z_copy(layer, z, far).start()
            return 0

        lax.fori_loop(1, lanes, step_z, 0)
        then()
        y_copy(layer, far).wait_recv()
        total = two(layer, far, lane) + yrecv[layer, far].astype(F32)
        for k in range(1, lanes):
            z = lax.rem(far + lanes - k, lanes)
            z_copy(layer, far, z).wait_recv()
            total = total + zrecv[layer, z].astype(F32)
        return total

    def gathered(layer):
        return mixed if layer else normed.at[1]

    def piece_copy(layer, z, y, device, send):
        ref = gathered(layer).at[rows_at(core, z, y)]
        return to(device, ref, ref, send, g_recv.at[layer, 2 * z + y])

    def z_piece(layer, z, owner):
        return piece_copy(layer, owner, lane, at_far(z), g_send.at[layer, z])

    def y_piece(layer, z, y):
        return piece_copy(layer, z, y, beside, b_send.at[layer, z])

    def core_piece(layer, z, y, c):
        ref = gathered(layer).at[rows_at(c, z, y)]
        return to(sibling, ref, ref, h_send.at[layer, 2 * z + y], h_recv.at[layer, 2 * z + y])

    def gather(layer, then):
        def send_z(k, _):
            z_piece(layer, lax.rem(far + k, lanes), far).start()
            return 0

        lax.fori_loop(1, lanes, send_z, 0)
        then()
        y_piece(layer, far, lane).start()
        core_piece(layer, far, lane, core).start()

        def pass_z(k, _):
            z = lax.rem(far + lanes - k, lanes)
            z_piece(layer, far, z).wait_recv()
            y_piece(layer, z, lane).start()
            core_piece(layer, z, lane, core).start()
            return 0

        lax.fori_loop(1, lanes, pass_z, 0)

        def pass_y(k, _):
            z = lax.rem(far + lanes - k, lanes)
            y_piece(layer, z, 1 - lane).wait_recv()
            core_piece(layer, z, 1 - lane, core).start()
            return 0

        lax.fori_loop(0, lanes, pass_y, 0)

        def land(k, _):
            core_piece(layer, k // 2, lax.rem(k, 2), 1 - core).wait_recv()
            return 0

        lax.fori_loop(0, chips, land, 0)

    def more(own_from, own_to, first, last):
        def act():
            hand_out(1, own_from, own_to)
            pass_on(1, first, last)

        return act

    def rest():
        return None

    for i in range(2):
        partial_copy(i).wait_recv()
    hide_one()
    hand_out(1, 0, 2)
    collect(0)
    project(0)
    total = reduce(0, more(2, 5, 0, 3))
    value = (x[own, :].astype(F32) + 0.5 * total).astype(BF16)
    middle[...] = value
    normed[1, own, :] = unit(value.astype(F32))
    gather(0, more(5, per_half, 3, per_half))
    wide_copy(2).wait_recv()
    wide_copy(3).wait_recv()
    hide_two()
    collect(1)
    project(1)
    total = reduce(1, rest)
    mixed[own, :] = (middle[...].astype(F32) + 0.5 * total).astype(BF16)
    gather(1, rest)

    wide_copy(0).wait_recv()
    wide_copy(1).wait_recv()
    for i in range(4):
        wide_copy(i).wait_send()
    for i in range(2):
        partial_copy(i).wait_send()
    guest_in.wait_send()
    guest_copy(beside, lane, core, 1).wait_send()
    guest_copy(sibling, lane, core, 2).wait_send()
    guest_copy(sibling, 1 - lane, core, 3).wait_send()
    for layer in range(2):

        def drain(k, _):
            block_copy(layer, lax.rem(t + k, n_tp), t).wait_send()
            return 0

        lax.fori_loop(1, n_tp, drain, 0)

        def drain_x(k, _):
            tall_copy(layer, turn(f, k)).wait_send()
            return 0

        lax.fori_loop(0, per_half, drain_x, 0)
        swap(layer, 0).wait_send()
        swap(layer, 1).wait_send()

        def drain_z(k, _):
            z = lax.rem(far + k, lanes)
            z_copy(layer, z, far).wait_send()
            z_piece(layer, z, far).wait_send()
            return 0

        lax.fori_loop(1, lanes, drain_z, 0)

        def drain_y(z, _):
            y_copy(layer, z).wait_send()
            y_piece(layer, z, lane).wait_send()
            return 0

        lax.fori_loop(0, lanes, drain_y, 0)

        def drain_c(k, _):
            core_piece(layer, k // 2, lax.rem(k, 2), core).wait_send()
            return 0

        lax.fori_loop(0, chips, drain_c, 0)


def flush(*refs):
    n = len(refs) // 2
    copies = [
        pltpu.make_async_copy(src, dst, refs[-1].at[i])
        for i, (src, dst) in enumerate(zip(refs[:n], refs[n : 2 * n]))
    ]
    for copy in copies:
        copy.start()
    for copy in copies:
        copy.wait()


def fused(n_tp, x, gain1, gate1, up1, down1, gain2, gate2, up2, down2):
    depth, width = gate1.shape
    tall_half, col = down1.shape
    tokens, model = x.shape
    block = 2 * tall_half // n_tp
    chips = n_tp // 2
    lanes = chips // 2
    side = tokens // 2
    piece = side // chips
    dma = pltpu.SemaphoreType.DMA
    vmem = pltpu.VMEM
    anywhere = pl.BlockSpec(memory_space=pl.ANY)
    wide_out = vmem((width, 2 * depth), BF16)
    down_out = vmem((block, model), BF16)
    held = pl.pallas_call(
        functools.partial(kernel, n_tp),
        out_shape=(vmem(x.shape, BF16), wide_out, wide_out, down_out, wide_out, wide_out, down_out),
        in_specs=[anywhere] * 9,
        out_specs=[pl.BlockSpec(memory_space=pltpu.VMEM)] * 7,
        scratch_shapes=[
            vmem((tokens, model), BF16),
            vmem((2, 1, depth), F32),
            vmem((4, width, depth), F32),
            vmem((2, tall_half, col), F32),
            vmem((2, 2 * tall_half, col), BF16),
            vmem((2, tokens, model), BF16),
            vmem((tokens, depth), BF16),
            vmem((2, tokens, width), BF16),
            vmem((2, tokens, width), BF16),
            vmem((2, tokens, width), F32),
            vmem((tokens, width), BF16),
            vmem((2, tokens, model), BF16),
            vmem((2, side, model), BF16),
            vmem((2, lanes, piece, model), BF16),
            vmem((2, lanes, piece, model), BF16),
            vmem((2, lanes, piece, model), BF16),
            vmem((2, lanes, piece, model), BF16),
            vmem((piece, model), BF16),
            dma((9,)), dma((4,)), dma((4,)), dma((2, n_tp)), dma((2, n_tp)), dma((6,)), dma((6,)),
            dma((2, n_tp)), dma((2, n_tp)),
            dma((2, 2)), dma((2, 2)), dma((2, lanes)), dma((2, lanes)), dma((2, lanes)), dma((2, lanes)),
            dma((2, lanes)), dma((2, chips)), dma((2, lanes)), dma((2, chips)), dma((2, chips)),
        ],
        compiler_params=pltpu.CompilerParams(
            collective_id=0, has_side_effects=True, vmem_limit_bytes=54 * 1024 * 1024
        ),
        name="hand_over",
    )(x, gain1[None, :], gate1.T, up1.T, down1, gain2[None, :], gate2.T, up2.T, down2)
    mixed, gate_one, up_one, down_one, gate_two, up_two, down_two = pl.pallas_call(
        flush,
        out_shape=tuple(jax.ShapeDtypeStruct(v.shape, v.dtype) for v in held),
        in_specs=[anywhere] * 7,
        out_specs=[anywhere] * 7,
        scratch_shapes=[dma((7,))],
        compiler_params=pltpu.CompilerParams(vmem_limit_bytes=1024 * 1024),
        name="flush",
    )(*held)
    return (mixed, gate_one.T, up_one.T, down_one, gate_two.T, up_two.T, down_two)


def solution(mesh):
    placed = (
        P(("grp", "fs"), None),
        P("fs"),
        P("fs", "tp"),
        P("fs", "tp"),
        P("fs", "tp"),
        P("fs"),
        P("fs", "tp"),
        P("fs", "tp"),
        P("fs", "tp"),
    )
    paired = mesh.shape["fs"] == 2 and mesh.shape["tp"] % 4 == 0
    return jax.shard_map(
        functools.partial(fused, mesh.shape["tp"]) if paired else body,
        mesh=mesh,
        in_specs=placed,
        out_specs=(
            P(("grp", "fs"), None),
            P("grp", "tp"),
            P("grp", "tp"),
            P(("grp", "tp"), None),
            P("grp", "tp"),
            P("grp", "tp"),
            P(("grp", "tp"), None),
        ),
        check_vma=False,
    )
```

```python
import functools

import jax
import jax.numpy as jnp
from jax import lax
from jax.experimental import pallas as pl
from jax.experimental.pallas import tpu as pltpu
from jax.sharding import PartitionSpec as P

MESH = pl.DeviceIdType.MESH
BF16 = jnp.bfloat16
F32 = jnp.float32

EPS = 1e-06


def serve_weights(gain, gate_w, up_w, down_w):
    gate_half = (gain[:, None] * gate_w).astype(jnp.bfloat16)
    up_half = (gain[:, None] * up_w).astype(jnp.bfloat16)
    down_half = down_w.astype(jnp.bfloat16)
    gate_whole, up_whole = (
        lax.all_gather(gate_half, "fs", axis=0, tiled=True),
        lax.all_gather(up_half, "fs", axis=0, tiled=True),
    )
    tall_block = lax.all_gather(down_half, "fs", axis=0, tiled=True)
    down_whole = lax.all_to_all(tall_block, "tp", split_axis=0, concat_axis=1, tiled=True)
    return (gate_whole, up_whole, down_whole)


def half_step(row_block, gate_w, up_w, down_w):
    values = row_block.astype(jnp.float32)
    normed = (values * lax.rsqrt(jnp.mean(values * values, axis=-1, keepdims=True) + EPS)).astype(
        jnp.bfloat16
    )
    gate_pre = jnp.dot(normed, gate_w, preferred_element_type=jnp.float32)
    up_pre = jnp.dot(normed, up_w, preferred_element_type=jnp.float32)
    hidden = (jax.nn.silu(gate_pre) * up_pre).astype(jnp.bfloat16)
    total = lax.psum(
        jnp.dot(hidden, down_w, preferred_element_type=jnp.float32).astype(jnp.bfloat16), "tp"
    ).astype(jnp.float32)
    return (values + 0.5 * total).astype(jnp.bfloat16)


def body(
    prompt_rows,
    gain_before,
    gate_before,
    up_before,
    down_before,
    gain_after,
    gate_after,
    up_after,
    down_after,
):
    gate_one, up_one, down_one = serve_weights(gain_before, gate_before, up_before, down_before)
    gate_two, up_two, down_two = serve_weights(gain_after, gate_after, up_after, down_after)
    middle = half_step(prompt_rows, gate_one, up_one, down_one)
    mixed = half_step(middle, gate_two, up_two, down_two)
    return (mixed, gate_one, up_one, down_one, gate_two, up_two, down_two)


def rows_of(start, size, unit):
    return pl.ds(pl.multiple_of(start, unit), size)


def kernel(
    n_tp,
    x_hbm, gain1_hbm, gate1_hbm, up1_hbm, down1_hbm, gain2_hbm, gate2_hbm, up2_hbm, down2_hbm,
    mixed, gate1, up1, down1, gate2, up2, down2,
    x, gain, wide, tall_in, tall, normed, guest, psend, precv, kept, hidden, part, pair,
    ysend, yrecv, zsend, zrecv, middle,
    in_sem, x_send, x_recv, d_send, d_recv, v_send, v_recv, a_send, a_recv, p_send, p_recv, y_send, y_recv, s_send, s_recv,
    g_send, g_recv, b_send, h_send, h_recv,
):
    f = lax.axis_index("fs")
    t = lax.axis_index("tp")
    other = 1 - f
    core = lax.rem(t, 2)
    chip = t // 2
    sibling = t + 1 - 2 * core
    chips = n_tp // 2
    width, depth = wide.shape[1:]
    tall_half = tall_in.shape[1]
    served = (gate1, up1, gate2, up2)
    down = (down1, down2)
    block = down1.shape[0]
    col = tall.shape[2]
    tokens = x.shape[0]
    side = tokens // 2
    piece = side // chips
    per_half = n_tp // 2
    eighth = per_half // 8
    own_cuts = (2 * eighth, 5 * eighth, per_half)
    cross_cuts = (0, 3 * eighth, per_half)
    lanes = chips // 2
    far = chip // 2
    lane = lax.rem(chip, 2)

    loads = {}
    sources = (
        ("x", x_hbm, x), ("down1", down1_hbm, tall_in.at[0]), ("gain1", gain1_hbm, gain.at[0]),
        ("gate1", gate1_hbm, wide.at[0]), ("up1", up1_hbm, wide.at[1]),
        ("down2", down2_hbm, tall_in.at[1]), ("gain2", gain2_hbm, gain.at[1]),
        ("gate2", gate2_hbm, wide.at[2]), ("up2", up2_hbm, wide.at[3]),
    )
    for i, (name, src, dst) in enumerate(sources):
        loads[name] = pltpu.make_async_copy(src, dst, in_sem.at[i])
        loads[name].start()

    barrier = pltpu.get_barrier_semaphore()
    for k in range(1, n_tp):
        pl.semaphore_signal(
            barrier, inc=1, device_id={"fs": f, "tp": lax.rem(t + k, n_tp)}, device_id_type=MESH
        )
    pl.semaphore_signal(barrier, inc=1, device_id={"fs": other, "tp": t}, device_id_type=MESH)
    def unit(v):
        return (v * lax.rsqrt(jnp.mean(v * v, axis=-1, keepdims=True) + EPS)).astype(BF16)

    def norm(k, _):
        rows = rows_of(k * 32, 32, 32)
        normed[0, rows, :] = unit(x[rows, :].astype(F32))
        return 0

    loads["x"].wait()
    lax.fori_loop(0, tokens // 32, norm, 0)

    near = rows_of(f * depth, depth, depth)
    away = rows_of(other * depth, depth, depth)

    def across(src, dst, send, recv):
        return pltpu.make_async_remote_copy(
            src_ref=src, dst_ref=dst, send_sem=send, recv_sem=recv,
            device_id={"fs": other, "tp": t}, device_id_type=MESH,
        )

    def to(tp, src, dst, send, recv):
        return pltpu.make_async_remote_copy(
            src_ref=src, dst_ref=dst, send_sem=send, recv_sem=recv,
            device_id={"fs": f, "tp": tp}, device_id_type=MESH,
        )

    def wide_copy(i):
        ref = served[i].at[:, near]
        return across(ref, ref, x_send.at[i], x_recv.at[i])

    def fold_wide(i, gain_slot):
        def one(k, _):
            rows = rows_of(k * 32, 32, 32)
            served[i][rows, near] = (gain[gain_slot] * wide[i, rows, :]).astype(BF16)
            return 0

        lax.fori_loop(0, width // 32, one, 0)

    def fold_tall(layer):
        step = tall_half // 8

        def one(k, _):
            tall[layer, rows_of(f * tall_half + k * step, step, 16), :] = tall_in[
                layer, rows_of(k * step, step, 16), :
            ].astype(BF16)
            return 0

        lax.fori_loop(0, 8, one, 0)

    my_cols = pl.ds(pl.multiple_of(t * col, col), col)

    def block_copy(layer, b, sender):
        return to(
            b, tall.at[layer, rows_of(b * block, block, 16)], down[layer].at[:, my_cols],
            a_send.at[layer, b], a_recv.at[layer, sender],
        )

    def tall_copy(layer, b):
        ref = tall.at[layer, rows_of(b * block, block, 16)]
        return across(ref, ref, d_send.at[layer, b], d_recv.at[layer, b])

    def turn(which, k):
        y = lax.rem(lane + k // lanes, 2)
        z = lax.rem(far + k // 2, lanes // 2)
        return which * per_half + (2 * z + y) * 2 + lax.rem(core + k, 2)

    def cross_tall(layer, first, last):
        def one(k, _):
            tall_copy(layer, turn(f, k)).start()
            return 0

        lax.fori_loop(first, last, one, 0)

    def hand_out(layer, first, last):
        def one(k, _):
            b = turn(f, k)

            @pl.when(b != t)
            def _():
                block_copy(layer, b, t).start()

            return 0

        lax.fori_loop(first, last, one, 0)

    def pass_on(layer, first, last):
        def one(k, _):
            b = turn(other, k)
            tall_copy(layer, b).wait_recv()

            @pl.when(b != t)
            def _():
                block_copy(layer, b, t).start()

            return 0

        lax.fori_loop(first, last, one, 0)

    def collect(layer):
        def one(k, _):
            block_copy(layer, t, lax.rem(t + k, n_tp)).wait_recv()
            return 0

        lax.fori_loop(1, n_tp, one, 0)
        down[layer][:, my_cols] = tall[layer, rows_of(t * block, block, 16), :]

    beside = 2 * (2 * far + 1 - lane) + core
    quarter = tokens // 4

    def share(y, c):
        return rows_of((2 * y + c) * quarter, quarter, quarter)

    guest_in = across(
        normed.at[0, share(lane, core), away], guest.at[share(lane, core)], v_send.at[0], v_recv.at[0]
    )

    def guest_copy(device, y, c, slot):
        ref = guest.at[share(y, c)]
        return to(device, ref, ref, v_send.at[slot], v_recv.at[slot])

    loads["down1"].wait()
    fold_tall(0)
    pl.semaphore_wait(barrier, n_tp)
    cross_tall(0, 0, eighth)
    guest_in.start()
    cross_tall(0, eighth, per_half)
    hand_out(0, 0, 4 * eighth)
    loads["gain1"].wait()
    loads["gate1"].wait()
    fold_wide(0, 0)
    loads["up1"].wait()
    fold_wide(1, 0)
    pass_on(0, 0, eighth)
    guest_in.wait_recv()
    guest_copy(beside, lane, core, 1).start()
    guest_copy(sibling, lane, core, 2).start()
    loads["down2"].wait()
    fold_tall(1)
    loads["gain2"].wait()
    loads["gate2"].wait()
    fold_wide(2, 1)
    loads["up2"].wait()
    fold_wide(3, 1)
    pass_on(0, eighth, 3 * eighth)
    guest_copy(beside, 1 - lane, core, 1).wait_recv()
    guest_copy(sibling, 1 - lane, core, 3).start()
    pass_on(0, 3 * eighth, 4 * eighth)
    guest_copy(sibling, lane, 1 - core, 2).wait_recv()
    guest_copy(sibling, 1 - lane, 1 - core, 3).wait_recv()
    hand_out(0, 4 * eighth, per_half)

    turned = (((1,), (1,)), ((), ()))

    def times(rows, i, cols):
        return lax.dot_general(rows, served[i][:, cols], turned, preferred_element_type=F32)

    def partial_copy(i):
        return across(psend.at[i], precv.at[i], v_send.at[4 + i], v_recv.at[4 + i])

    for i in range(2):
        psend[i] = times(guest[...], i, near).astype(BF16)
        partial_copy(i).start()
    cross_tall(1, 0, per_half)
    for i in (2, 3, 0, 1):
        wide_copy(i).start()
    pass_on(0, 4 * eighth, 6 * eighth)
    for i in range(2):
        kept[i] = times(normed[0, :, near], i, near)
    pass_on(0, 6 * eighth, per_half)

    def gated(rows, g, u):
        hidden[rows, :] = (g / (1.0 + jnp.exp(-g)) * u).astype(BF16)

    def hide_one():
        def one(k, _):
            rows = rows_of(k * 32, 32, 32)
            gated(rows, kept[0, rows, :] + precv[0, rows, :].astype(F32),
                  kept[1, rows, :] + precv[1, rows, :].astype(F32))
            return 0

        lax.fori_loop(0, tokens // 32, one, 0)

    def hide_two():
        gated(slice(None), times(normed[1], 2, slice(None)), times(normed[1], 3, slice(None)))

    def peer(k):
        m = k + lanes // 2 - 1
        m = jnp.where(m < lanes, m, jnp.where(k == lanes, 0, m - lanes + 1))
        return lax.bitwise_xor(far, m)

    def spot(z, y):
        return (y * lanes + z) * piece

    def rows_at(c, z, y):
        return rows_of(c * side + spot(z, y), piece, piece)

    def at_far(z):
        return 2 * (2 * z + lane) + core

    def swap(layer, y):
        half = side // 2
        src = part.at[layer, rows_of((1 - core) * side + y * half, half, half)]
        return to(sibling, src, pair.at[layer, rows_of(y * half, half, half)],
                  p_send.at[layer, y], p_recv.at[layer, y])

    def y_copy(layer, z):
        return to(beside, ysend.at[layer, z], yrecv.at[layer, z], y_send.at[layer, z], y_recv.at[layer, z])

    def z_copy(layer, z, sender):
        return to(at_far(z), zsend.at[layer, z], zrecv.at[layer, sender],
                  s_send.at[layer, z], s_recv.at[layer, sender])

    own = rows_at(core, far, lane)

    def project(layer):
        def rows_for(c):
            rows = rows_of(c * side, side, side)
            p = jnp.dot(hidden[rows, :], down[layer][...], preferred_element_type=F32)
            part[layer, rows, :] = p.astype(BF16)

        rows_for(1 - core)
        swap(layer, 1 - lane).start()
        swap(layer, lane).start()
        rows_for(core)

    def two(layer, z, y):
        return part[layer, rows_at(core, z, y), :].astype(F32) + pair[
            layer, rows_of(spot(z, y), piece, piece), :
        ].astype(F32)

    def reduce(layer, then):
        swap(layer, 1 - lane).wait_recv()

        def step_y(k, _):
            z = peer(k)
            ysend[layer, z] = two(layer, z, 1 - lane).astype(BF16)
            y_copy(layer, z).start()
            return 0

        lax.fori_loop(1, lanes + 1, step_y, 0)
        swap(layer, lane).wait_recv()

        def step_z(k, _):
            z = peer(k)
            y_copy(layer, z).wait_recv()
            zsend[layer, z] = (two(layer, z, lane) + yrecv[layer, z].astype(F32)).astype(BF16)
            z_copy(layer, z, far).start()
            return 0

        lax.fori_loop(1, lanes, step_z, 0)
        then(0)
        y_copy(layer, far).wait_recv()
        total = two(layer, far, lane) + yrecv[layer, far].astype(F32)
        for k in range(1, lanes):
            z = peer(k)
            z_copy(layer, far, z).wait_recv()
            total = total + zrecv[layer, z].astype(F32)
        return total

    def gathered(layer):
        return mixed if layer else normed.at[1]

    def piece_copy(layer, z, y, device, send):
        ref = gathered(layer).at[rows_at(core, z, y)]
        return to(device, ref, ref, send, g_recv.at[layer, 2 * z + y])

    def z_piece(layer, z, owner):
        return piece_copy(layer, owner, lane, at_far(z), g_send.at[layer, z])

    def y_piece(layer, z, y):
        return piece_copy(layer, z, y, beside, b_send.at[layer, z])

    def core_piece(layer, z, y, c):
        ref = gathered(layer).at[rows_at(c, z, y)]
        return to(sibling, ref, ref, h_send.at[layer, 2 * z + y], h_recv.at[layer, 2 * z + y])

    def gather(layer, then):
        def send_z(k, _):
            z_piece(layer, peer(k), far).start()
            return 0

        lax.fori_loop(1, lanes, send_z, 0)
        then(1)
        y_piece(layer, far, lane).start()
        core_piece(layer, far, lane, core).start()

        def pass_z(k, _):
            z = peer(k)
            z_piece(layer, far, z).wait_recv()
            y_piece(layer, z, lane).start()
            core_piece(layer, z, lane, core).start()
            then(1 + k)
            return 0

        lax.fori_loop(1, lanes, pass_z, 0)

        def pass_y(k, _):
            z = peer(jnp.where(k == 0, lanes, k))
            y_piece(layer, z, 1 - lane).wait_recv()
            core_piece(layer, z, 1 - lane, core).start()
            then(1 + lanes + k)
            return 0

        lax.fori_loop(0, lanes, pass_y, 0)

        def land(k, _):
            core_piece(layer, k // 2, lax.rem(k, 2), 1 - core).wait_recv()
            return 0

        lax.fori_loop(0, chips, land, 0)

    def dole(k):
        if isinstance(k, int) and k + 1 < len(own_cuts):
            hand_out(1, own_cuts[k], own_cuts[k + 1])
            pass_on(1, cross_cuts[k], cross_cuts[k + 1])

    def rest(k):
        return None

    for i in range(2):
        partial_copy(i).wait_recv()
    hide_one()
    hand_out(1, 0, own_cuts[0])
    collect(0)
    pass_on(1, 0, cross_cuts[0])
    project(0)
    total = reduce(0, dole)
    value = (x[own, :].astype(F32) + 0.5 * total).astype(BF16)
    middle[...] = value
    normed[1, own, :] = unit(value.astype(F32))
    gather(0, dole)
    hand_out(1, own_cuts[-1], per_half)
    pass_on(1, cross_cuts[-1], per_half)
    wide_copy(2).wait_recv()
    wide_copy(3).wait_recv()
    hide_two()
    collect(1)
    project(1)
    total = reduce(1, rest)
    mixed[own, :] = (middle[...].astype(F32) + 0.5 * total).astype(BF16)
    gather(1, rest)

    wide_copy(0).wait_recv()
    wide_copy(1).wait_recv()
    for i in range(4):
        wide_copy(i).wait_send()
    for i in range(2):
        partial_copy(i).wait_send()
    guest_in.wait_send()
    guest_copy(beside, lane, core, 1).wait_send()
    guest_copy(sibling, lane, core, 2).wait_send()
    guest_copy(sibling, 1 - lane, core, 3).wait_send()
    for layer in range(2):

        def drain(k, _):
            block_copy(layer, lax.rem(t + k, n_tp), t).wait_send()
            return 0

        lax.fori_loop(1, n_tp, drain, 0)

        def drain_x(k, _):
            tall_copy(layer, turn(f, k)).wait_send()
            return 0

        lax.fori_loop(0, per_half, drain_x, 0)
        swap(layer, 0).wait_send()
        swap(layer, 1).wait_send()

        def drain_z(k, _):
            z = lax.rem(far + k, lanes)
            z_copy(layer, z, far).wait_send()
            z_piece(layer, z, far).wait_send()
            return 0

        lax.fori_loop(1, lanes, drain_z, 0)

        def drain_y(z, _):
            y_copy(layer, z).wait_send()
            y_piece(layer, z, lane).wait_send()
            return 0

        lax.fori_loop(0, lanes, drain_y, 0)

        def drain_c(k, _):
            core_piece(layer, k // 2, lax.rem(k, 2), core).wait_send()
            return 0

        lax.fori_loop(0, chips, drain_c, 0)


def flush(*refs):
    n = len(refs) // 2
    copies = [
        pltpu.make_async_copy(src, dst, refs[-1].at[i])
        for i, (src, dst) in enumerate(zip(refs[:n], refs[n : 2 * n]))
    ]
    for copy in copies:
        copy.start()
    for copy in copies:
        copy.wait()


def fused(n_tp, x, gain1, gate1, up1, down1, gain2, gate2, up2, down2):
    depth, width = gate1.shape
    tall_half, col = down1.shape
    tokens, model = x.shape
    block = 2 * tall_half // n_tp
    chips = n_tp // 2
    lanes = chips // 2
    side = tokens // 2
    piece = side // chips
    dma = pltpu.SemaphoreType.DMA
    vmem = pltpu.VMEM
    anywhere = pl.BlockSpec(memory_space=pl.ANY)
    wide_out = vmem((width, 2 * depth), BF16)
    down_out = vmem((block, model), BF16)
    held = pl.pallas_call(
        functools.partial(kernel, n_tp),
        out_shape=(vmem(x.shape, BF16), wide_out, wide_out, down_out, wide_out, wide_out, down_out),
        in_specs=[anywhere] * 9,
        out_specs=[pl.BlockSpec(memory_space=pltpu.VMEM)] * 7,
        scratch_shapes=[
            vmem((tokens, model), BF16),
            vmem((2, 1, depth), F32),
            vmem((4, width, depth), F32),
            vmem((2, tall_half, col), F32),
            vmem((2, 2 * tall_half, col), BF16),
            vmem((2, tokens, model), BF16),
            vmem((tokens, depth), BF16),
            vmem((2, tokens, width), BF16),
            vmem((2, tokens, width), BF16),
            vmem((2, tokens, width), F32),
            vmem((tokens, width), BF16),
            vmem((2, tokens, model), BF16),
            vmem((2, side, model), BF16),
            vmem((2, lanes, piece, model), BF16),
            vmem((2, lanes, piece, model), BF16),
            vmem((2, lanes, piece, model), BF16),
            vmem((2, lanes, piece, model), BF16),
            vmem((piece, model), BF16),
            dma((9,)), dma((4,)), dma((4,)), dma((2, n_tp)), dma((2, n_tp)), dma((6,)), dma((6,)),
            dma((2, n_tp)), dma((2, n_tp)),
            dma((2, 2)), dma((2, 2)), dma((2, lanes)), dma((2, lanes)), dma((2, lanes)), dma((2, lanes)),
            dma((2, lanes)), dma((2, chips)), dma((2, lanes)), dma((2, chips)), dma((2, chips)),
        ],
        compiler_params=pltpu.CompilerParams(
            collective_id=0, has_side_effects=True, vmem_limit_bytes=54 * 1024 * 1024
        ),
        name="hand_over",
    )(x, gain1[None, :], gate1.T, up1.T, down1, gain2[None, :], gate2.T, up2.T, down2)
    mixed, gate_one, up_one, down_one, gate_two, up_two, down_two = pl.pallas_call(
        flush,
        out_shape=tuple(jax.ShapeDtypeStruct(v.shape, v.dtype) for v in held),
        in_specs=[anywhere] * 7,
        out_specs=[anywhere] * 7,
        scratch_shapes=[dma((7,))],
        compiler_params=pltpu.CompilerParams(vmem_limit_bytes=1024 * 1024),
        name="flush",
    )(*held)
    return (mixed, gate_one.T, up_one.T, down_one, gate_two.T, up_two.T, down_two)


def solution(mesh):
    placed = (
        P(("grp", "fs"), None),
        P("fs"),
        P("fs", "tp"),
        P("fs", "tp"),
        P("fs", "tp"),
        P("fs"),
        P("fs", "tp"),
        P("fs", "tp"),
        P("fs", "tp"),
    )
    tp = mesh.shape["tp"]
    paired = mesh.shape["fs"] == 2 and tp % 16 == 0 and tp & (tp - 1) == 0
    return jax.shard_map(
        functools.partial(fused, tp) if paired else body,
        mesh=mesh,
        in_specs=placed,
        out_specs=(
            P(("grp", "fs"), None),
            P("grp", "tp"),
            P("grp", "tp"),
            P(("grp", "tp"), None),
            P("grp", "tp"),
            P("grp", "tp"),
            P(("grp", "tp"), None),
        ),
        check_vma=False,
    )
```

```python
import functools

import jax
import jax.numpy as jnp
from jax import lax
from jax.experimental import pallas as pl
from jax.experimental.pallas import tpu as pltpu
from jax.sharding import PartitionSpec as P

MESH = pl.DeviceIdType.MESH
BF16 = jnp.bfloat16
F32 = jnp.float32

EPS = 1e-06


def serve_weights(gain, gate_w, up_w, down_w):
    gate_half = (gain[:, None] * gate_w).astype(jnp.bfloat16)
    up_half = (gain[:, None] * up_w).astype(jnp.bfloat16)
    down_half = down_w.astype(jnp.bfloat16)
    gate_whole, up_whole = (
        lax.all_gather(gate_half, "fs", axis=0, tiled=True),
        lax.all_gather(up_half, "fs", axis=0, tiled=True),
    )
    tall_block = lax.all_gather(down_half, "fs", axis=0, tiled=True)
    down_whole = lax.all_to_all(tall_block, "tp", split_axis=0, concat_axis=1, tiled=True)
    return (gate_whole, up_whole, down_whole)


def half_step(row_block, gate_w, up_w, down_w):
    values = row_block.astype(jnp.float32)
    normed = (values * lax.rsqrt(jnp.mean(values * values, axis=-1, keepdims=True) + EPS)).astype(
        jnp.bfloat16
    )
    gate_pre = jnp.dot(normed, gate_w, preferred_element_type=jnp.float32)
    up_pre = jnp.dot(normed, up_w, preferred_element_type=jnp.float32)
    hidden = (jax.nn.silu(gate_pre) * up_pre).astype(jnp.bfloat16)
    total = lax.psum(
        jnp.dot(hidden, down_w, preferred_element_type=jnp.float32).astype(jnp.bfloat16), "tp"
    ).astype(jnp.float32)
    return (values + 0.5 * total).astype(jnp.bfloat16)


def body(
    prompt_rows,
    gain_before,
    gate_before,
    up_before,
    down_before,
    gain_after,
    gate_after,
    up_after,
    down_after,
):
    gate_one, up_one, down_one = serve_weights(gain_before, gate_before, up_before, down_before)
    gate_two, up_two, down_two = serve_weights(gain_after, gate_after, up_after, down_after)
    middle = half_step(prompt_rows, gate_one, up_one, down_one)
    mixed = half_step(middle, gate_two, up_two, down_two)
    return (mixed, gate_one, up_one, down_one, gate_two, up_two, down_two)


def rows_of(start, size, unit):
    return pl.ds(pl.multiple_of(start, unit), size)


def kernel(
    n_tp,
    x_hbm, gain1_hbm, gate1_hbm, up1_hbm, down1_hbm, gain2_hbm, gate2_hbm, up2_hbm, down2_hbm,
    mixed, gate1, up1, down1, gate2, up2, down2,
    x, gain, wide, tall_in, tall, normed, guest, psend, precv, kept, hidden, part, pair,
    ysend, yrecv, zsend, zrecv, middle,
    in_sem, x_send, x_recv, d_send, d_recv, v_send, v_recv, a_send, a_recv, p_send, p_recv,
    y_send, y_recv, s_send, s_recv,
    g_send, g_recv, b_send, h_send, h_recv,
):
    f = lax.axis_index("fs")
    t = lax.axis_index("tp")
    other = 1 - f
    core = lax.rem(t, 2)
    chip = t // 2
    sibling = t + 1 - 2 * core
    chips = n_tp // 2
    width, depth = wide.shape[1:]
    tall_half = tall_in.shape[1]
    served = (gate1, up1, gate2, up2)
    down = (down1, down2)
    block = down1.shape[0]
    col = tall.shape[2]
    tokens = x.shape[0]
    side = tokens // 2
    piece = side // chips
    per_half = n_tp // 2
    eighth = per_half // 8
    own_cuts = (2 * eighth, 5 * eighth, per_half)
    cross_cuts = (0, 3 * eighth, per_half)
    lanes = chips // 2
    far = chip // 2
    lane = lax.rem(chip, 2)

    barrier = pltpu.get_barrier_semaphore()
    for k in range(1, n_tp):
        pl.semaphore_signal(
            barrier, inc=1, device_id={"fs": f, "tp": lax.rem(t + k, n_tp)}, device_id_type=MESH
        )
    pl.semaphore_signal(barrier, inc=1, device_id={"fs": other, "tp": t}, device_id_type=MESH)

    loads = {}
    sources = (
        ("down1", down1_hbm, tall_in.at[0]), ("x", x_hbm, x), ("gain1", gain1_hbm, gain.at[0]),
        ("gate1", gate1_hbm, wide.at[0]), ("up1", up1_hbm, wide.at[1]),
        ("down2", down2_hbm, tall_in.at[1]), ("gain2", gain2_hbm, gain.at[1]),
        ("gate2", gate2_hbm, wide.at[2]), ("up2", up2_hbm, wide.at[3]),
    )
    for i, (name, src, dst) in enumerate(sources):
        loads[name] = pltpu.make_async_copy(src, dst, in_sem.at[i])
        loads[name].start()

    def unit(v):
        return (v * lax.rsqrt(jnp.mean(v * v, axis=-1, keepdims=True) + EPS)).astype(BF16)

    def norm(k, _):
        rows = rows_of(k * 32, 32, 32)
        normed[0, rows, :] = unit(x[rows, :].astype(F32))
        return 0

    near = rows_of(f * depth, depth, depth)
    away = rows_of(other * depth, depth, depth)

    def across(src, dst, send, recv):
        return pltpu.make_async_remote_copy(
            src_ref=src, dst_ref=dst, send_sem=send, recv_sem=recv,
            device_id={"fs": other, "tp": t}, device_id_type=MESH,
        )

    def to(tp, src, dst, send, recv):
        return pltpu.make_async_remote_copy(
            src_ref=src, dst_ref=dst, send_sem=send, recv_sem=recv,
            device_id={"fs": f, "tp": tp}, device_id_type=MESH,
        )

    def wide_copy(i):
        ref = served[i].at[:, near]
        return across(ref, ref, x_send.at[i], x_recv.at[i])

    def fold_wide(i, gain_slot):
        def one(k, _):
            rows = rows_of(k * 32, 32, 32)
            served[i][rows, near] = (gain[gain_slot] * wide[i, rows, :]).astype(BF16)
            return 0

        lax.fori_loop(0, width // 32, one, 0)

    def fold_tall(layer):
        step = tall_half // 8

        def one(k, _):
            tall[layer, rows_of(f * tall_half + k * step, step, 16), :] = tall_in[
                layer, rows_of(k * step, step, 16), :
            ].astype(BF16)
            return 0

        lax.fori_loop(0, 8, one, 0)

    my_cols = pl.ds(pl.multiple_of(t * col, col), col)

    def block_copy(layer, b):
        return to(
            b, tall.at[layer, rows_of(b * block, block, 16)], down[layer].at[:, my_cols],
            a_send.at[layer], a_recv.at[layer],
        )

    def tall_copy(layer, b):
        ref = tall.at[layer, rows_of(b * block, block, 16)]
        return across(ref, ref, d_send.at[layer], d_recv.at[layer, lax.rem(b, per_half)])

    def turn(which, k):
        y = lax.rem(lane + k // lanes, 2)
        z = lax.rem(far + k // 2, lanes // 2)
        return which * per_half + (2 * z + y) * 2 + lax.rem(core + k, 2)

    def cross_tall(layer, first, last):
        def one(k, _):
            tall_copy(layer, turn(f, k)).start()
            return 0

        lax.fori_loop(first, last, one, 0)

    def hand_out(layer, first, last):
        def one(k, _):
            b = turn(f, k)

            @pl.when(b != t)
            def _():
                block_copy(layer, b).start()

            return 0

        lax.fori_loop(first, last, one, 0)

    def pass_on(layer, first, last):
        def one(k, _):
            b = turn(other, k)
            tall_copy(layer, b).wait_recv()

            @pl.when(b != t)
            def _():
                block_copy(layer, b).start()

            return 0

        lax.fori_loop(first, last, one, 0)

    def all_blocks(layer):
        ref = down[layer].at[:, pl.ds(0, (n_tp - 1) * col)]
        return to(sibling, ref, ref, a_send.at[layer], a_recv.at[layer])

    def collect(layer):
        all_blocks(layer).wait_recv()
        down[layer][:, my_cols] = tall[layer, rows_of(t * block, block, 16), :]

    beside = 2 * (2 * far + 1 - lane) + core
    quarter = tokens // 4

    def share(y, c):
        return rows_of((2 * y + c) * quarter, quarter, quarter)

    guest_in = across(
        normed.at[0, share(lane, core), away], guest.at[share(lane, core)], v_send.at[0], v_recv.at[0]
    )

    def guest_copy(device, y, c, slot):
        ref = guest.at[share(y, c)]
        return to(device, ref, ref, v_send.at[slot], v_recv.at[slot])

    loads["down1"].wait()
    fold_tall(0)
    pl.semaphore_wait(barrier, n_tp)
    cross_tall(0, 0, eighth)
    hand_out(0, 0, 4 * eighth)
    loads["x"].wait()
    lax.fori_loop(0, tokens // 32, norm, 0)
    guest_in.start()
    cross_tall(0, eighth, per_half)
    loads["gain1"].wait()
    loads["gate1"].wait()
    fold_wide(0, 0)
    loads["up1"].wait()
    fold_wide(1, 0)
    pass_on(0, 0, eighth)
    guest_in.wait_recv()
    guest_copy(beside, lane, core, 1).start()
    guest_copy(sibling, lane, core, 2).start()
    loads["down2"].wait()
    fold_tall(1)
    loads["gain2"].wait()
    loads["gate2"].wait()
    fold_wide(2, 1)
    loads["up2"].wait()
    fold_wide(3, 1)
    pass_on(0, eighth, 3 * eighth)
    guest_copy(beside, 1 - lane, core, 1).wait_recv()
    guest_copy(sibling, 1 - lane, core, 3).start()
    pass_on(0, 3 * eighth, 4 * eighth)
    guest_copy(sibling, lane, 1 - core, 2).wait_recv()
    guest_copy(sibling, 1 - lane, 1 - core, 3).wait_recv()
    hand_out(0, 4 * eighth, per_half)

    turned = (((1,), (1,)), ((), ()))

    def times(rows, i, cols):
        return lax.dot_general(rows, served[i][:, cols], turned, preferred_element_type=F32)

    def partial_copy(i):
        return across(psend.at[i], precv.at[i], v_send.at[4 + i], v_recv.at[4 + i])

    for i in range(2):
        psend[i] = times(guest[...], i, near).astype(BF16)
        partial_copy(i).start()
    cross_tall(1, 0, per_half)
    for i in (2, 3, 0, 1):
        wide_copy(i).start()
    pass_on(0, 4 * eighth, 6 * eighth)
    for i in range(2):
        kept[i] = times(normed[0, :, near], i, near)
    pass_on(0, 6 * eighth, per_half)

    def gated(rows, g, u):
        hidden[rows, :] = (g / (1.0 + jnp.exp(-g)) * u).astype(BF16)

    def hide_one():
        def one(k, _):
            rows = rows_of(k * 32, 32, 32)
            gated(rows, kept[0, rows, :] + precv[0, rows, :].astype(F32),
                  kept[1, rows, :] + precv[1, rows, :].astype(F32))
            return 0

        lax.fori_loop(0, tokens // 32, one, 0)

    def hide_two():
        gated(slice(None), times(normed[1], 2, slice(None)), times(normed[1], 3, slice(None)))

    near_z = lax.bitwise_xor(far, 1)
    over_z = lax.bitwise_xor(far, 2)
    last_z = lax.bitwise_xor(far, 3)

    def spot(z, y):
        return (y * lanes + z) * piece

    def rows_at(c, z, y):
        return rows_of(c * side + spot(z, y), piece, piece)

    def at_far(z):
        return 2 * (2 * z + lane) + core

    def swap(layer, y):
        half = side // 2
        src = part.at[layer, rows_of((1 - core) * side + y * half, half, half)]
        return to(sibling, src, pair.at[layer, rows_of(y * half, half, half)],
                  p_send.at[layer], p_recv.at[layer, y])

    def y_copy(layer, z):
        return to(beside, ysend.at[layer, z], yrecv.at[layer, z], y_send.at[layer], y_recv.at[layer, z])

    def z_copy(layer, z, device, slot):
        return to(at_far(device), zsend.at[layer, z], zrecv.at[layer, slot],
                  s_send.at[layer], s_recv.at[layer, slot])

    own = rows_at(core, far, lane)

    def project(layer):
        def rows_for(c):
            rows = rows_of(c * side, side, side)
            p = jnp.dot(hidden[rows, :], down[layer][...], preferred_element_type=F32)
            part[layer, rows, :] = p.astype(BF16)

        rows_for(1 - core)
        swap(layer, 1 - lane).start()
        swap(layer, lane).start()
        rows_for(core)

    def two(layer, z, y):
        return part[layer, rows_at(core, z, y), :].astype(F32) + pair[
            layer, rows_of(spot(z, y), piece, piece), :
        ].astype(F32)

    def reduce(layer, then):
        swap(layer, 1 - lane).wait_recv()

        for z in (last_z, near_z, over_z, far):
            ysend[layer, z] = two(layer, z, 1 - lane).astype(BF16)
            y_copy(layer, z).start()
        swap(layer, lane).wait_recv()

        def summed(z):
            y_copy(layer, z).wait_recv()
            return two(layer, z, lane) + yrecv[layer, z].astype(F32)

        for z in (last_z, near_z):
            zsend[layer, z] = summed(z).astype(BF16)
            z_copy(layer, z, near_z, z).start()
        total = summed(over_z)
        z_copy(layer, far, far, over_z).wait_recv()
        zsend[layer, over_z] = (total + zrecv[layer, over_z].astype(F32)).astype(BF16)
        z_copy(layer, over_z, over_z, last_z).start()
        then(0)
        total = summed(far)
        for slot in (far, near_z):
            z_copy(layer, far, far, slot).wait_recv()
            total = total + zrecv[layer, slot].astype(F32)
        return total

    def gathered(layer):
        return mixed if layer else normed.at[1]

    def piece_copy(layer, z, y, device, send):
        ref = gathered(layer).at[rows_at(core, z, y)]
        return to(device, ref, ref, send, g_recv.at[layer, 2 * z + y])

    def z_piece(layer, owner, device):
        return piece_copy(layer, owner, lane, at_far(device), g_send.at[layer])

    def y_piece(layer, z, y):
        return piece_copy(layer, z, y, beside, b_send.at[layer])

    def core_piece(layer, z, y, c):
        ref = gathered(layer).at[rows_at(c, z, y)]
        return to(sibling, ref, ref, h_send.at[layer], h_recv.at[layer])

    def gather(layer, then):
        z_piece(layer, far, over_z).start()
        z_piece(layer, far, near_z).start()
        if layer == 0:
            then(1)
        y_piece(layer, far, lane).start()
        core_piece(layer, far, lane, core).start()
        if layer:
            then(1)
        for z in (over_z, near_z, last_z):
            z_piece(layer, z, near_z).wait_recv()
            if z is over_z:
                z_piece(layer, z, near_z).start()
            y_piece(layer, z, lane).start()
            core_piece(layer, z, lane, core).start()
        for z in (far, over_z, near_z, last_z):
            y_piece(layer, z, 1 - lane).wait_recv()
            core_piece(layer, z, 1 - lane, core).start()

        ref = gathered(layer).at[rows_of((1 - core) * side, side, side)]
        to(sibling, ref, ref, h_send.at[layer], h_recv.at[layer]).wait_recv()

    def dole(k):
        if isinstance(k, int) and k + 1 < len(own_cuts):
            hand_out(1, own_cuts[k], own_cuts[k + 1])
            pass_on(1, cross_cuts[k], cross_cuts[k + 1])

    def drain_blocks(layer):
        all_blocks(layer).wait_send()
        ref = tall.at[layer, rows_of(f * tall_half, tall_half, 16)]
        across(ref, ref, d_send.at[layer], d_recv.at[layer, 0]).wait_send()

    def drain_sum(layer):
        to(sibling, pair.at[layer], pair.at[layer], p_send.at[layer], p_recv.at[layer, 0]).wait_send()
        three = zsend.at[layer, pl.ds(0, 3)]
        to(sibling, three, three, s_send.at[layer], s_recv.at[layer, 0]).wait_send()
        four = ysend.at[layer]
        to(beside, four, four, y_send.at[layer], y_recv.at[layer, 0]).wait_send()

    def drain_gather(layer):
        three, four, eight = zsend.at[layer, pl.ds(0, 3)], ysend.at[layer], pair.at[layer]
        to(sibling, three, three, g_send.at[layer], g_recv.at[layer, 0]).wait_send()
        to(beside, four, four, b_send.at[layer], g_recv.at[layer, 0]).wait_send()
        to(sibling, eight, eight, h_send.at[layer], h_recv.at[layer]).wait_send()

    def settle(k):
        if k == 0:
            drain_blocks(0)
            drain_blocks(1)
        if k == 1:
            drain_sum(0)
            drain_gather(0)
            for i in range(2):
                wide_copy(2 + i).wait_send()
                partial_copy(i).wait_send()
            guest_in.wait_send()
            guest_copy(beside, lane, core, 1).wait_send()
            guest_copy(sibling, lane, core, 2).wait_send()
            guest_copy(sibling, 1 - lane, core, 3).wait_send()

    for i in range(2):
        partial_copy(i).wait_recv()
    hide_one()
    hand_out(1, 0, own_cuts[0])
    collect(0)
    pass_on(1, 0, cross_cuts[0])
    project(0)
    total = reduce(0, dole)
    value = (x[own, :].astype(F32) + 0.5 * total).astype(BF16)
    middle[...] = value
    normed[1, own, :] = unit(value.astype(F32))
    gather(0, dole)
    hand_out(1, own_cuts[-1], per_half)
    pass_on(1, cross_cuts[-1], per_half)
    wide_copy(2).wait_recv()
    wide_copy(3).wait_recv()
    hide_two()
    collect(1)
    project(1)
    total = reduce(1, settle)
    mixed[own, :] = (middle[...].astype(F32) + 0.5 * total).astype(BF16)
    gather(1, settle)

    drain_sum(1)
    drain_gather(1)
    for i in range(2):
        wide_copy(i).wait_recv()
        wide_copy(i).wait_send()


def flush(*refs):
    n = len(refs) // 2
    copies = [
        pltpu.make_async_copy(src, dst, refs[-1].at[i])
        for i, (src, dst) in enumerate(zip(refs[:n], refs[n : 2 * n]))
    ]
    for copy in copies:
        copy.start()
    for copy in copies:
        copy.wait()


def fused(n_tp, x, gain1, gate1, up1, down1, gain2, gate2, up2, down2):
    depth, width = gate1.shape
    tall_half, col = down1.shape
    tokens, model = x.shape
    block = 2 * tall_half // n_tp
    chips = n_tp // 2
    lanes = chips // 2
    side = tokens // 2
    piece = side // chips
    dma = pltpu.SemaphoreType.DMA
    vmem = pltpu.VMEM
    anywhere = pl.BlockSpec(memory_space=pl.ANY)
    wide_out = vmem((width, 2 * depth), BF16)
    down_out = vmem((block, model), BF16)
    held = pl.pallas_call(
        functools.partial(kernel, n_tp),
        out_shape=(vmem(x.shape, BF16), wide_out, wide_out, down_out, wide_out, wide_out, down_out),
        in_specs=[anywhere] * 9,
        out_specs=[pl.BlockSpec(memory_space=pltpu.VMEM)] * 7,
        scratch_shapes=[
            vmem((tokens, model), BF16),
            vmem((2, 1, depth), F32),
            vmem((4, width, depth), F32),
            vmem((2, tall_half, col), F32),
            vmem((2, 2 * tall_half, col), BF16),
            vmem((2, tokens, model), BF16),
            vmem((tokens, depth), BF16),
            vmem((2, tokens, width), BF16),
            vmem((2, tokens, width), BF16),
            vmem((2, tokens, width), F32),
            vmem((tokens, width), BF16),
            vmem((2, tokens, model), BF16),
            vmem((2, side, model), BF16),
            vmem((2, lanes, piece, model), BF16),
            vmem((2, lanes, piece, model), BF16),
            vmem((2, lanes, piece, model), BF16),
            vmem((2, lanes, piece, model), BF16),
            vmem((piece, model), BF16),
            dma((9,)), dma((4,)), dma((4,)), dma((2,)), dma((2, n_tp // 2)), dma((6,)), dma((6,)),
            dma((2,)), dma((2,)), dma((2,)), dma((2, 2)), dma((2,)), dma((2, lanes)),
            dma((2,)), dma((2, lanes)), dma((2,)), dma((2, chips)), dma((2,)), dma((2,)), dma((2,)),
        ],
        compiler_params=pltpu.CompilerParams(
            collective_id=0, has_side_effects=True, vmem_limit_bytes=54 * 1024 * 1024
        ),
        name="hand_over",
    )(x, gain1[None, :], gate1.T, up1.T, down1, gain2[None, :], gate2.T, up2.T, down2)
    mixed, gate_one, up_one, down_one, gate_two, up_two, down_two = pl.pallas_call(
        flush,
        out_shape=tuple(jax.ShapeDtypeStruct(v.shape, v.dtype) for v in held),
        in_specs=[anywhere] * 7,
        out_specs=[anywhere] * 7,
        scratch_shapes=[dma((7,))],
        compiler_params=pltpu.CompilerParams(vmem_limit_bytes=1024 * 1024),
        name="flush",
    )(*held)
    return (mixed, gate_one.T, up_one.T, down_one, gate_two.T, up_two.T, down_two)


def solution(mesh):
    placed = (
        P(("grp", "fs"), None),
        P("fs"),
        P("fs", "tp"),
        P("fs", "tp"),
        P("fs", "tp"),
        P("fs"),
        P("fs", "tp"),
        P("fs", "tp"),
        P("fs", "tp"),
    )
    tp = mesh.shape["tp"]
    paired = mesh.shape["fs"] == 2 and tp // 4 == 4 and tp % 4 == 0
    return jax.shard_map(
        functools.partial(fused, tp) if paired else body,
        mesh=mesh,
        in_specs=placed,
        out_specs=(
            P(("grp", "fs"), None),
            P("grp", "tp"),
            P("grp", "tp"),
            P(("grp", "tp"), None),
            P("grp", "tp"),
            P("grp", "tp"),
            P(("grp", "tp"), None),
        ),
        check_vma=False,
    )
```

```python
import functools

import jax
import jax.numpy as jnp
from jax import lax
from jax.experimental import pallas as pl
from jax.experimental.pallas import tpu as pltpu
from jax.sharding import PartitionSpec as P

MESH = pl.DeviceIdType.MESH
BF16 = jnp.bfloat16
F32 = jnp.float32

EPS = 1e-06


def serve_weights(gain, gate_w, up_w, down_w):
    gate_half = (gain[:, None] * gate_w).astype(jnp.bfloat16)
    up_half = (gain[:, None] * up_w).astype(jnp.bfloat16)
    down_half = down_w.astype(jnp.bfloat16)
    gate_whole, up_whole = (
        lax.all_gather(gate_half, "fs", axis=0, tiled=True),
        lax.all_gather(up_half, "fs", axis=0, tiled=True),
    )
    tall_block = lax.all_gather(down_half, "fs", axis=0, tiled=True)
    down_whole = lax.all_to_all(tall_block, "tp", split_axis=0, concat_axis=1, tiled=True)
    return (gate_whole, up_whole, down_whole)


def half_step(row_block, gate_w, up_w, down_w):
    values = row_block.astype(jnp.float32)
    normed = (values * lax.rsqrt(jnp.mean(values * values, axis=-1, keepdims=True) + EPS)).astype(
        jnp.bfloat16
    )
    gate_pre = jnp.dot(normed, gate_w, preferred_element_type=jnp.float32)
    up_pre = jnp.dot(normed, up_w, preferred_element_type=jnp.float32)
    hidden = (jax.nn.silu(gate_pre) * up_pre).astype(jnp.bfloat16)
    total = lax.psum(
        jnp.dot(hidden, down_w, preferred_element_type=jnp.float32).astype(jnp.bfloat16), "tp"
    ).astype(jnp.float32)
    return (values + 0.5 * total).astype(jnp.bfloat16)


def body(
    prompt_rows,
    gain_before,
    gate_before,
    up_before,
    down_before,
    gain_after,
    gate_after,
    up_after,
    down_after,
):
    gate_one, up_one, down_one = serve_weights(gain_before, gate_before, up_before, down_before)
    gate_two, up_two, down_two = serve_weights(gain_after, gate_after, up_after, down_after)
    middle = half_step(prompt_rows, gate_one, up_one, down_one)
    mixed = half_step(middle, gate_two, up_two, down_two)
    return (mixed, gate_one, up_one, down_one, gate_two, up_two, down_two)


def rows_of(start, size, unit):
    return pl.ds(pl.multiple_of(start, unit), size)


def kernel(
    n_tp,
    x_hbm, gain1_hbm, gate1_hbm, up1_hbm, down1_hbm, gain2_hbm, gate2_hbm, up2_hbm, down2_hbm,
    mixed, gate1, up1, down1, gate2, up2, down2,
    x, gain, wide, tall_in, tall, normed, guest, psend, precv, kept, upright, hidden, part, pair,
    ysend, yrecv, zsend, zrecv, middle,
    in_sem, x_send, x_recv, d_send, d_recv, v_send, v_recv, a_send, a_recv, p_send, p_recv,
    y_send, y_recv, s_send, s_recv,
    g_send, g_recv, b_send, h_send, h_recv,
):
    f = lax.axis_index("fs")
    t = lax.axis_index("tp")
    other = 1 - f
    core = lax.rem(t, 2)
    chip = t // 2
    sibling = t + 1 - 2 * core
    chips = n_tp // 2
    width, depth = wide.shape[1:]
    tall_half = tall_in.shape[1]
    served = (gate1, up1, gate2, up2)
    down = (down1, down2)
    block = down1.shape[0]
    col = tall.shape[2]
    tokens = x.shape[0]
    side = tokens // 2
    piece = side // chips
    per_half = n_tp // 2
    eighth = per_half // 8
    own_cuts = (2 * eighth, 5 * eighth, per_half)
    cross_cuts = (eighth, 4 * eighth, per_half)
    lanes = chips // 2
    far = chip // 2
    lane = lax.rem(chip, 2)

    barrier = pltpu.get_barrier_semaphore()
    for k in range(1, n_tp):
        pl.semaphore_signal(
            barrier, inc=1, device_id={"fs": f, "tp": lax.rem(t + k, n_tp)}, device_id_type=MESH
        )
    pl.semaphore_signal(barrier, inc=1, device_id={"fs": other, "tp": t}, device_id_type=MESH)

    loads = {}
    sources = (
        ("down1", down1_hbm, tall_in.at[0]), ("x", x_hbm, x), ("gain1", gain1_hbm, gain.at[0]),
        ("gate1", gate1_hbm, wide.at[0]), ("up1", up1_hbm, wide.at[1]),
        ("down2", down2_hbm, tall_in.at[1]), ("gain2", gain2_hbm, gain.at[1]),
        ("gate2", gate2_hbm, wide.at[2]), ("up2", up2_hbm, wide.at[3]),
    )
    for i, (name, src, dst) in enumerate(sources):
        loads[name] = pltpu.make_async_copy(src, dst, in_sem.at[i])
        loads[name].start()

    def unit(v):
        return (v * lax.rsqrt(jnp.mean(v * v, axis=-1, keepdims=True) + EPS)).astype(BF16)

    def norm(k, _):
        rows = rows_of(k * 32, 32, 32)
        normed[0, rows, :] = unit(x[rows, :].astype(F32))
        return 0

    near = rows_of(f * depth, depth, depth)
    away = rows_of(other * depth, depth, depth)

    def across(src, dst, send, recv):
        return pltpu.make_async_remote_copy(
            src_ref=src, dst_ref=dst, send_sem=send, recv_sem=recv,
            device_id={"fs": other, "tp": t}, device_id_type=MESH,
        )

    def to(tp, src, dst, send, recv):
        return pltpu.make_async_remote_copy(
            src_ref=src, dst_ref=dst, send_sem=send, recv_sem=recv,
            device_id={"fs": f, "tp": tp}, device_id_type=MESH,
        )

    def wide_copy(i):
        ref = served[i].at[:, near]
        return across(ref, ref, x_send.at[i], x_recv.at[i])

    def fold_wide(i, gain_slot):
        def one(k, _):
            rows = rows_of(k * 32, 32, 32)
            served[i][rows, near] = (gain[gain_slot] * wide[i, rows, :]).astype(BF16)
            return 0

        lax.fori_loop(0, width // 32, one, 0)

    def fold_tall(layer):
        step = tall_half // 8

        def one(k, _):
            tall[layer, rows_of(f * tall_half + k * step, step, 16), :] = tall_in[
                layer, rows_of(k * step, step, 16), :
            ].astype(BF16)
            return 0

        lax.fori_loop(0, 8, one, 0)

    my_cols = pl.ds(pl.multiple_of(t * col, col), col)

    def block_copy(layer, b):
        return to(
            b, tall.at[layer, rows_of(b * block, block, 16)], down[layer].at[:, my_cols],
            a_send.at[layer], a_recv.at[layer],
        )

    def tall_copy(layer, b):
        ref = tall.at[layer, rows_of(b * block, block, 16)]
        return across(ref, ref, d_send.at[layer], d_recv.at[layer, lax.rem(b, per_half)])

    def turn(which, k):
        y = lax.rem(lane + k // lanes, 2)
        z = lax.rem(far + k // 2, lanes // 2)
        return which * per_half + (2 * z + y) * 2 + lax.rem(core + k, 2)

    def cross_tall(layer, first, last):
        def one(k, _):
            tall_copy(layer, turn(f, k)).start()
            return 0

        lax.fori_loop(first, last, one, 0)

    def hand_out(layer, first, last):
        def one(k, _):
            b = turn(f, k)

            @pl.when(b != t)
            def _():
                block_copy(layer, b).start()

            return 0

        lax.fori_loop(first, last, one, 0)

    def pass_on(layer, first, last):
        def one(k, _):
            b = turn(other, k)
            tall_copy(layer, b).wait_recv()

            @pl.when(b != t)
            def _():
                block_copy(layer, b).start()

            return 0

        lax.fori_loop(first, last, one, 0)

    def all_blocks(layer):
        ref = down[layer].at[:, pl.ds(0, (n_tp - 1) * col)]
        return to(sibling, ref, ref, a_send.at[layer], a_recv.at[layer])

    def collect(layer):
        all_blocks(layer).wait_recv()
        down[layer][:, my_cols] = tall[layer, rows_of(t * block, block, 16), :]

    beside = 2 * (2 * far + 1 - lane) + core
    quarter = tokens // 4

    def share(y, c):
        return rows_of((2 * y + c) * quarter, quarter, quarter)

    guest_in = across(
        normed.at[0, share(lane, core), away], guest.at[share(lane, core)], v_send.at[0], v_recv.at[0]
    )

    def guest_copy(device, y, c, slot):
        ref = guest.at[share(y, c)]
        return to(device, ref, ref, v_send.at[slot], v_recv.at[slot])

    loads["down1"].wait()
    fold_tall(0)
    pl.semaphore_wait(barrier, n_tp)
    cross_tall(0, 0, eighth)
    hand_out(0, 0, 4 * eighth)
    loads["x"].wait()
    lax.fori_loop(0, tokens // 32, norm, 0)
    guest_in.start()
    cross_tall(0, eighth, per_half)
    loads["gain1"].wait()
    loads["gate1"].wait()
    fold_wide(0, 0)
    loads["up1"].wait()
    fold_wide(1, 0)
    pass_on(0, 0, eighth)
    guest_in.wait_recv()
    guest_copy(beside, lane, core, 1).start()
    guest_copy(sibling, lane, core, 2).start()
    loads["down2"].wait()
    fold_tall(1)
    loads["gain2"].wait()
    loads["gate2"].wait()
    fold_wide(2, 1)
    loads["up2"].wait()
    fold_wide(3, 1)
    pass_on(0, eighth, 3 * eighth)
    guest_copy(beside, 1 - lane, core, 1).wait_recv()
    guest_copy(sibling, 1 - lane, core, 3).start()
    pass_on(0, 3 * eighth, 4 * eighth)
    guest_copy(sibling, lane, 1 - core, 2).wait_recv()
    guest_copy(sibling, 1 - lane, 1 - core, 3).wait_recv()
    hand_out(0, 4 * eighth, per_half)

    turned = (((1,), (1,)), ((), ()))

    def times(rows, i, cols):
        return lax.dot_general(rows, served[i][:, cols], turned, preferred_element_type=F32)

    def partial_copy(i):
        return across(psend.at[i], precv.at[i], v_send.at[4 + i], v_recv.at[4 + i])

    for i in range(2):
        psend[i] = lax.dot_general(
            served[i][:, near], guest[...], turned, preferred_element_type=F32
        ).astype(BF16)
        partial_copy(i).start()
    cross_tall(1, 0, per_half)
    for i in (2, 3, 0, 1):
        wide_copy(i).start()
    pass_on(0, 4 * eighth, 6 * eighth)
    for i in range(2):
        kept[i] = lax.dot_general(
            served[i][:, near], normed[0, :, near], turned, preferred_element_type=F32
        )
    pass_on(0, 6 * eighth, per_half)

    def gated(g, u):
        return (g / (1.0 + jnp.exp(-g)) * u).astype(BF16)

    def hide_one():
        def one(k, _):
            rows = rows_of(k * 32, 32, 32)
            upright[rows, :] = gated(
                kept[0, rows, :] + precv[0, rows, :].astype(F32),
                kept[1, rows, :] + precv[1, rows, :].astype(F32),
            )
            return 0

        lax.fori_loop(0, width // 32, one, 0)

    def hide_two():
        whole = slice(None)
        hidden[...] = gated(times(normed[1], 2, whole), times(normed[1], 3, whole))

    near_z = lax.bitwise_xor(far, 1)
    over_z = lax.bitwise_xor(far, 2)
    last_z = lax.bitwise_xor(far, 3)

    def spot(z, y):
        return (y * lanes + z) * piece

    def rows_at(c, z, y):
        return rows_of(c * side + spot(z, y), piece, piece)

    def at_far(z):
        return 2 * (2 * z + lane) + core

    def swap(layer, y):
        half = side // 2
        src = part.at[layer, rows_of((1 - core) * side + y * half, half, half)]
        return to(sibling, src, pair.at[layer, rows_of(y * half, half, half)],
                  p_send.at[layer], p_recv.at[layer, y])

    def y_copy(layer, z):
        return to(beside, ysend.at[layer, z], yrecv.at[layer, z], y_send.at[layer], y_recv.at[layer, z])

    def z_copy(layer, z, device, slot):
        return to(at_far(device), zsend.at[layer, z], zrecv.at[layer, slot],
                  s_send.at[layer], s_recv.at[layer, slot])

    own = rows_at(core, far, lane)

    def project(layer):
        def rows_for(c):
            rows = rows_of(c * side, side, side)
            if layer:
                p = jnp.dot(hidden[rows, :], down2[...], preferred_element_type=F32)
            else:
                p = lax.dot_general(
                    upright[:, rows], down1[...], (((0,), (0,)), ((), ())), preferred_element_type=F32
                )
            part[layer, rows, :] = p.astype(BF16)

        rows_for(1 - core)
        swap(layer, 1 - lane).start()
        swap(layer, lane).start()
        rows_for(core)

    def two(layer, z, y):
        return part[layer, rows_at(core, z, y), :].astype(F32) + pair[
            layer, rows_of(spot(z, y), piece, piece), :
        ].astype(F32)

    def reduce(layer, then):
        swap(layer, 1 - lane).wait_recv()

        for z in (last_z, near_z, over_z, far):
            ysend[layer, z] = two(layer, z, 1 - lane).astype(BF16)
            y_copy(layer, z).start()
        swap(layer, lane).wait_recv()

        def summed(z):
            y_copy(layer, z).wait_recv()
            return two(layer, z, lane) + yrecv[layer, z].astype(F32)

        for z in (last_z, near_z):
            zsend[layer, z] = summed(z).astype(BF16)
            z_copy(layer, z, near_z, z).start()
        total = summed(over_z)
        z_copy(layer, far, far, over_z).wait_recv()
        zsend[layer, over_z] = (total + zrecv[layer, over_z].astype(F32)).astype(BF16)
        z_copy(layer, over_z, over_z, last_z).start()
        then(0)
        total = summed(far)
        for slot in (far, near_z):
            z_copy(layer, far, far, slot).wait_recv()
            total = total + zrecv[layer, slot].astype(F32)
        return total

    def gathered(layer):
        return mixed if layer else normed.at[1]

    def piece_copy(layer, z, y, device, send):
        ref = gathered(layer).at[rows_at(core, z, y)]
        return to(device, ref, ref, send, g_recv.at[layer, 2 * z + y])

    def z_piece(layer, owner, device):
        return piece_copy(layer, owner, lane, at_far(device), g_send.at[layer])

    def y_piece(layer, z, y):
        return piece_copy(layer, z, y, beside, b_send.at[layer])

    def core_piece(layer, z, y, c):
        ref = gathered(layer).at[rows_at(c, z, y)]
        return to(sibling, ref, ref, h_send.at[layer], h_recv.at[layer])

    def gather(layer, then):
        z_piece(layer, far, over_z).start()
        z_piece(layer, far, near_z).start()
        if layer == 0:
            then(1)
        y_piece(layer, far, lane).start()
        core_piece(layer, far, lane, core).start()
        if layer:
            then(1)
        for z in (over_z, near_z, last_z):
            z_piece(layer, z, near_z).wait_recv()
            if z is over_z:
                z_piece(layer, z, near_z).start()
            y_piece(layer, z, lane).start()
            core_piece(layer, z, lane, core).start()
        for z in (far, over_z, near_z, last_z):
            y_piece(layer, z, 1 - lane).wait_recv()
            core_piece(layer, z, 1 - lane, core).start()

        ref = gathered(layer).at[rows_of((1 - core) * side, side, side)]
        to(sibling, ref, ref, h_send.at[layer], h_recv.at[layer]).wait_recv()

    def dole(k):
        if isinstance(k, int) and k + 1 < len(own_cuts):
            hand_out(1, own_cuts[k], own_cuts[k + 1])
            pass_on(1, cross_cuts[k], cross_cuts[k + 1])

    def drain_blocks(layer):
        all_blocks(layer).wait_send()
        ref = tall.at[layer, rows_of(f * tall_half, tall_half, 16)]
        across(ref, ref, d_send.at[layer], d_recv.at[layer, 0]).wait_send()

    def drain_sum(layer):
        to(sibling, pair.at[layer], pair.at[layer], p_send.at[layer], p_recv.at[layer, 0]).wait_send()
        three = zsend.at[layer, pl.ds(0, 3)]
        to(sibling, three, three, s_send.at[layer], s_recv.at[layer, 0]).wait_send()
        four = ysend.at[layer]
        to(beside, four, four, y_send.at[layer], y_recv.at[layer, 0]).wait_send()

    def drain_gather(layer):
        three, four, eight = zsend.at[layer, pl.ds(0, 3)], ysend.at[layer], pair.at[layer]
        to(sibling, three, three, g_send.at[layer], g_recv.at[layer, 0]).wait_send()
        to(beside, four, four, b_send.at[layer], g_recv.at[layer, 0]).wait_send()
        to(sibling, eight, eight, h_send.at[layer], h_recv.at[layer]).wait_send()

    def settle(k):
        if k == 0:
            drain_blocks(0)
            drain_blocks(1)
        if k == 1:
            drain_sum(0)
            drain_gather(0)
            for i in range(2):
                wide_copy(2 + i).wait_send()
                partial_copy(i).wait_send()
            guest_in.wait_send()
            guest_copy(beside, lane, core, 1).wait_send()
            guest_copy(sibling, lane, core, 2).wait_send()
            guest_copy(sibling, 1 - lane, core, 3).wait_send()

    for i in range(2):
        partial_copy(i).wait_recv()
    hide_one()
    hand_out(1, 0, own_cuts[0])
    collect(0)
    pass_on(1, 0, cross_cuts[0])
    project(0)
    total = reduce(0, dole)
    value = (x[own, :].astype(F32) + 0.5 * total).astype(BF16)
    middle[...] = value
    normed[1, own, :] = unit(value.astype(F32))
    gather(0, dole)
    hand_out(1, own_cuts[-1], per_half)
    pass_on(1, cross_cuts[-1], per_half)
    wide_copy(2).wait_recv()
    wide_copy(3).wait_recv()
    hide_two()
    collect(1)
    project(1)
    total = reduce(1, settle)
    mixed[own, :] = (middle[...].astype(F32) + 0.5 * total).astype(BF16)
    gather(1, settle)

    drain_sum(1)
    drain_gather(1)
    for i in range(2):
        wide_copy(i).wait_recv()
        wide_copy(i).wait_send()


def flush(*refs):
    n = len(refs) // 2
    copies = [
        pltpu.make_async_copy(src, dst, refs[-1].at[i])
        for i, (src, dst) in enumerate(zip(refs[:n], refs[n : 2 * n]))
    ]
    for copy in copies:
        copy.start()
    for copy in copies:
        copy.wait()


def fused(n_tp, x, gain1, gate1, up1, down1, gain2, gate2, up2, down2):
    depth, width = gate1.shape
    tall_half, col = down1.shape
    tokens, model = x.shape
    block = 2 * tall_half // n_tp
    chips = n_tp // 2
    lanes = chips // 2
    side = tokens // 2
    piece = side // chips
    dma = pltpu.SemaphoreType.DMA
    vmem = pltpu.VMEM
    anywhere = pl.BlockSpec(memory_space=pl.ANY)
    wide_out = vmem((width, 2 * depth), BF16)
    down_out = vmem((block, model), BF16)
    held = pl.pallas_call(
        functools.partial(kernel, n_tp),
        out_shape=(vmem(x.shape, BF16), wide_out, wide_out, down_out, wide_out, wide_out, down_out),
        in_specs=[anywhere] * 9,
        out_specs=[pl.BlockSpec(memory_space=pltpu.VMEM)] * 7,
        scratch_shapes=[
            vmem((tokens, model), BF16),
            vmem((2, 1, depth), F32),
            vmem((4, width, depth), F32),
            vmem((2, tall_half, col), F32),
            vmem((2, 2 * tall_half, col), BF16),
            vmem((2, tokens, model), BF16),
            vmem((tokens, depth), BF16),
            vmem((2, width, tokens), BF16),
            vmem((2, width, tokens), BF16),
            vmem((2, width, tokens), F32),
            vmem((width, tokens), BF16),
            vmem((tokens, width), BF16),
            vmem((2, tokens, model), BF16),
            vmem((2, side, model), BF16),
            vmem((2, lanes, piece, model), BF16),
            vmem((2, lanes, piece, model), BF16),
            vmem((2, lanes, piece, model), BF16),
            vmem((2, lanes, piece, model), BF16),
            vmem((piece, model), BF16),
            dma((9,)), dma((4,)), dma((4,)), dma((2,)), dma((2, n_tp // 2)), dma((6,)), dma((6,)),
            dma((2,)), dma((2,)), dma((2,)), dma((2, 2)), dma((2,)), dma((2, lanes)),
            dma((2,)), dma((2, lanes)), dma((2,)), dma((2, chips)), dma((2,)), dma((2,)), dma((2,)),
        ],
        compiler_params=pltpu.CompilerParams(
            collective_id=0, has_side_effects=True, vmem_limit_bytes=54 * 1024 * 1024
        ),
        name="hand_over",
    )(x, gain1[None, :], gate1.T, up1.T, down1, gain2[None, :], gate2.T, up2.T, down2)
    mixed, gate_one, up_one, down_one, gate_two, up_two, down_two = pl.pallas_call(
        flush,
        out_shape=tuple(jax.ShapeDtypeStruct(v.shape, v.dtype) for v in held),
        in_specs=[anywhere] * 7,
        out_specs=[anywhere] * 7,
        scratch_shapes=[dma((7,))],
        compiler_params=pltpu.CompilerParams(vmem_limit_bytes=1024 * 1024),
        name="flush",
    )(*held)
    return (mixed, gate_one.T, up_one.T, down_one, gate_two.T, up_two.T, down_two)


def solution(mesh):
    placed = (
        P(("grp", "fs"), None),
        P("fs"),
        P("fs", "tp"),
        P("fs", "tp"),
        P("fs", "tp"),
        P("fs"),
        P("fs", "tp"),
        P("fs", "tp"),
        P("fs", "tp"),
    )
    tp = mesh.shape["tp"]
    paired = mesh.shape["fs"] == 2 and tp // 4 == 4 and tp % 4 == 0
    return jax.shard_map(
        functools.partial(fused, tp) if paired else body,
        mesh=mesh,
        in_specs=placed,
        out_specs=(
            P(("grp", "fs"), None),
            P("grp", "tp"),
            P("grp", "tp"),
            P(("grp", "tp"), None),
            P("grp", "tp"),
            P("grp", "tp"),
            P(("grp", "tp"), None),
        ),
        check_vma=False,
    )
```
